128 devices in a mesh: kv: 16 (over z, y), tp: 8 (over x, core).
Axes of the slice: x: 4, y: 4, z: 4, core: 2. Of those that a mesh axis runs over, the one named last changes fastest.
Arguments:
- tokens: bfloat16 [256, 4, 2048], P(None, None, ('kv', 'tp')), may hold values from -520 to 520
- input_norm_gain: bfloat16 [2048], replicated, may hold values from 0.099609375 to 1.8984375
- query_weight: bfloat16 [2048, 2048], P(None, 'kv'), may hold values from -0.125 to 0.125
- key_weight: bfloat16 [2048, 2048], P(None, 'kv'), may hold values from -0.125 to 0.125
- value_weight: bfloat16 [2048, 16, 128], P(None, 'kv', 'tp'), may hold values from -1.14904852 to 1.14904852
- output_gate_weight: bfloat16 [2048, 16, 128], P(None, 'kv', 'tp'), may hold values from -0.125 to 0.125
- strength_weight: bfloat16 [2048, 16], P(None, 'kv'), may hold values from -0.125 to 0.125
- decay_weight: bfloat16 [2048, 16], P(None, 'kv'), may hold values from -0.125 to 0.125
- head_decay_rate: float32 [16], P('kv'), may hold values from 0.005 to 1.5
- proposal_log_decay: float32 [256, 4, 16], P(None, None, 'kv'), may hold values from -0.69 to 0
- head_norm_gain: bfloat16 [128], P('tp'), may hold values from 0.099609375 to 1.8984375
- output_weight: bfloat16 [16, 128, 2048], P('kv', 'tp'), may hold values from -1.14904852 to 1.14904852
- output_norm_gain: bfloat16 [2048], P(('kv', 'tp')), may hold values from 0.099609375 to 1.8984375
- state: float32 [256, 16, 128, 128], P(None, 'kv', 'tp'), may hold values from -4.5961941 to 4.5961941
- previous_keys: bfloat16 [256, 4, 2048], P(None, None, 'kv'), may hold values from -6 to 6
- previous_values: bfloat16 [256, 4, 16, 128], P(None, None, 'kv', 'tp'), may hold values from -52 to 52
- previous_log_decay: float32 [256, 4, 16], P(None, None, 'kv'), may hold values from -0.7 to -0.02
- previous_strengths: float32 [256, 4, 16], P(None, None, 'kv'), may hold values from 0.1 to 0.9
- accepted: int32 [256], replicated, may hold values from 0 to 4
- parent: int32 [256, 4], replicated, may hold values from -1 to 2, as said below
Outputs:
- layer_out: bfloat16 [256, 4, 2048], P(None, None, ('kv', 'tp'))
- accepted_state: float32 [256, 16, 128, 128], P(None, 'kv', 'tp')
The draws below stay inside these ranges and needn't reach their ends.
Inputs may be any that keep to these rules, and one draw needn't show every extreme that they name: parent[b, i] is -1 or a proposal index below i; -1 means that proposal i follows the accepted old proposals directly.
All inputs are finite; a program needn't handle non-finite values.
Results may differ from the reference program's by a relative error of at most 0.019.
Values may be sent and summed in bfloat16 or wider, within the bound.
No kernel may reach another device: no remote copies, remote signals or barrier semaphores. Data moves between devices by JAX's collectives and lax.ppermute only.
A program may use at most 128 MiB of HBM per device.

```python
import jax
import jax.numpy as jnp
from jax import lax

D = 2048
H = 16
HD = 128
PROP = 4
SEQS = 256


def column_scales(key, count):
    position = jnp.arange(count, dtype=jnp.float32) / max(count - 1, 1)
    spread = jax.random.uniform(key, (count,), jnp.float32)
    return jnp.exp(jnp.log(3.0) * position + jnp.log(3.4) * spread)


def rough_base(key, shape):
    base = jax.random.normal(key, shape, jnp.float32)
    return jnp.clip(base, -5.0, 5.0)


def draw_tokens(key, part):
    subkeys = jax.random.split(jax.random.fold_in(key, 11), 3)
    base = rough_base(subkeys[0], (SEQS, PROP, D))
    rowscale = jnp.exp(jnp.log(10.0) * jax.random.uniform(subkeys[2], (SEQS, PROP, 1), jnp.float32))
    return (base * column_scales(subkeys[1], D)[None, None, :] * rowscale).astype(jnp.bfloat16)


def draw_output_weight(key, part):
    subkeys = jax.random.split(jax.random.fold_in(key, 23), 2)
    base = jax.random.normal(subkeys[0], (H, HD, D), jnp.float32)
    base = jnp.clip(base, -5.0, 5.0)
    scaled = base * (H * HD) ** (-0.5) * column_scales(subkeys[1], D)[None, None, :]
    return scaled.astype(jnp.bfloat16)


def draw_value_weight(key, part):
    subkeys = jax.random.split(jax.random.fold_in(key, 61), 2)
    base = rough_base(subkeys[0], (D, H, HD))
    return (base * D ** (-0.5) * column_scales(subkeys[1], HD)[None, None, :]).astype(jnp.bfloat16)


def draw_state(key, part):
    subkeys = jax.random.split(jax.random.fold_in(key, 67), 2)
    base = rough_base(subkeys[0], (SEQS, H, HD, HD))
    return base * HD ** (-0.5) * column_scales(subkeys[1], HD)[None, None, :, None]


def draw_previous_values(key, part):
    subkeys = jax.random.split(jax.random.fold_in(key, 71), 2)
    base = rough_base(subkeys[0], (SEQS, PROP, H, HD))
    return (base * column_scales(subkeys[1], HD)[None, None, None, :]).astype(jnp.bfloat16)


def draw_head_decay_rate(key, part):
    uniform_part = jax.random.uniform(jax.random.fold_in(key, 31), (H,), jnp.float32)
    lowest = 0.02
    highest = 1.5
    return jnp.exp(jnp.log(lowest) + uniform_part * (jnp.log(highest) - jnp.log(lowest)))


def draw_proposal_log_decay(key, part):
    subkeys = jax.random.split(jax.random.fold_in(key, 41), 2)
    chosen = (jax.random.randint(subkeys[0], (SEQS, PROP, H), 0, 4) == 0).astype(jnp.float32)
    depth = jax.random.uniform(subkeys[1], (SEQS, PROP, H), jnp.float32, 0.22, 0.69)
    return -depth * chosen


def draw_parent(key, part):
    raw_bits = jax.random.randint(jax.random.fold_in(key, 53), (SEQS, PROP), 0, 1 << 20)
    column = jnp.arange(PROP, dtype=jnp.int32)
    return (raw_bits % (column[None, :] + 1) - 1).astype(jnp.int32)


def set_ends(drawn, rng, low, top_value):
    extent = drawn.shape
    spot = [jax.random.randint(jax.random.fold_in(rng, axis), (), 0, extent[axis]) for axis in range(len(extent))]
    drawn = drawn.at[tuple(spot)].set(low)
    longest = extent.index(max(extent))
    spot[longest] = (spot[longest] + 1) % extent[longest]
    return drawn.at[tuple(spot)].set(top_value)


def levels(own_key, shape, shards, smallest, high):
    gain, own = 1.0, jax.random.fold_in(own_key, 6)
    for dim, parts in shards:
        draws = jnp.exp(jax.random.uniform(jax.random.fold_in(own, dim), (parts,), jnp.float32, smallest / len(shards), high / len(shards)))
        gain = gain * jnp.repeat(draws, shape[dim] // parts).reshape([-1 if axis == dim else 1 for axis in range(len(shape))])
    return gain


def normal_values(own_key, extent, scale, most, cuts=(), kind=jnp.bfloat16):
    values = scale * jax.random.normal(own_key, extent, jnp.float32)
    if cuts:
        values = values * levels(own_key, extent, cuts, -0.22, 0.18)
    return jnp.clip(values, -most, most).astype(kind)


def setup_inputs(seed: int = 0) -> dict:
    key_list = jax.random.split(jax.random.key(seed), 21)
    tokens = draw_tokens(jax.random.fold_in(key_list[20], 71), 0)
    input_norm_gain = jnp.clip(1.0 + 0.18 * jax.random.normal(key_list[1], (D,), jnp.float32), 0.099609375, 1.8984375).astype(jnp.bfloat16)
    query_weight = normal_values(key_list[2], (D, H * HD), D ** -0.5, 0.125, ((1, 16),))
    key_weight = normal_values(key_list[3], (D, H * HD), D ** -0.5, 0.125, ((1, 16),))
    value_weight = draw_value_weight(jax.random.fold_in(key_list[20], 71), 0)
    output_gate_weight = normal_values(key_list[5], (D, H, HD), D ** -0.5, 0.125, ((1, 16), (2, 8)))
    strength_weight = normal_values(key_list[6], (D, H), D ** -0.5, 0.125, ((1, 16),))
    decay_weight = normal_values(key_list[7], (D, H), D ** -0.5, 0.125, ((1, 16),))
    head_decay_rate = draw_head_decay_rate(jax.random.fold_in(key_list[20], 71), 0)
    proposal_log_decay = draw_proposal_log_decay(jax.random.fold_in(key_list[20], 71), 0)
    head_norm_gain = jnp.clip(1.0 + 0.18 * jax.random.normal(key_list[10], (HD,), jnp.float32), 0.099609375, 1.8984375).astype(jnp.bfloat16)
    output_weight = draw_output_weight(jax.random.fold_in(key_list[20], 71), 0)
    output_norm_gain = jnp.clip(1.0 + 0.18 * jax.random.normal(key_list[12], (D,), jnp.float32), 0.099609375, 1.8984375).astype(jnp.bfloat16)
    state = draw_state(jax.random.fold_in(key_list[20], 71), 0)
    previous_keys = normal_values(key_list[14], (SEQS, PROP, H * HD), 1.0, 6.0, ((2, 16),))
    previous_values = draw_previous_values(jax.random.fold_in(key_list[20], 71), 0)
    previous_log_decay = jnp.clip(-0.7 + 0.68 * jax.random.uniform(key_list[16], (SEQS, PROP, H), jnp.float32) ** levels(key_list[16], (SEQS, PROP, H), ((2, 16),), -0.2, 0.2), -0.7, -0.02)
    previous_strengths = jnp.clip(0.1 + 0.79999997 * jax.random.uniform(key_list[17], (SEQS, PROP, H), jnp.float32) ** levels(key_list[17], (SEQS, PROP, H), ((2, 16),), -0.2, 0.2), 0.1, 0.9)
    accepted = set_ends(jax.random.randint(key_list[18], (SEQS,), 0, PROP + 1), jax.random.fold_in(key_list[18], 1), 0, PROP).astype(jnp.int32)
    parent = draw_parent(jax.random.fold_in(key_list[20], 71), 0)
    return {"tokens": tokens, "input_norm_gain": input_norm_gain, "query_weight": query_weight, "key_weight": key_weight, "value_weight": value_weight, "output_gate_weight": output_gate_weight, "strength_weight": strength_weight, "decay_weight": decay_weight, "head_decay_rate": head_decay_rate, "proposal_log_decay": proposal_log_decay, "head_norm_gain": head_norm_gain, "output_weight": output_weight, "output_norm_gain": output_norm_gain, "state": state, "previous_keys": previous_keys, "previous_values": previous_values, "previous_log_decay": previous_log_decay, "previous_strengths": previous_strengths, "accepted": accepted, "parent": parent}


epsilon = 1e-06

def unit_rows(matrix):
    return matrix * lax.rsqrt(lax.optimization_barrier(jnp.sum(matrix * matrix, axis=-1, keepdims=True)) + epsilon)

def exact_product(form, left, right):
    return jnp.einsum(form, left, right, precision=lax.Precision.HIGHEST)

def visibility(parent):
    sequence_count, proposal_count = parent.shape
    position = jnp.arange(proposal_count, dtype=jnp.int32)
    parent_hot = (parent[:, :, None] == position[None, None, :]).astype(jnp.float32)
    ancestry = []
    for row_index in range(proposal_count):
        ancestor_row = parent_hot[:, row_index, :]
        if row_index > 0:
            earlier = jnp.stack(ancestry, axis=1)
            ancestor_row = ancestor_row + exact_product('bj,bjk->bk', parent_hot[:, row_index, :row_index], earlier)
        ancestry.append(ancestor_row)
    ancestor = jnp.stack(ancestry, axis=1)
    chain = (position[:, None] > position[None, :]).astype(jnp.float32)
    upper = jnp.concatenate([jnp.broadcast_to(chain, (sequence_count, proposal_count, proposal_count)), jnp.zeros((sequence_count, proposal_count, proposal_count), jnp.float32)], axis=2)
    lower = jnp.concatenate([jnp.ones((sequence_count, proposal_count, proposal_count), jnp.float32), ancestor], axis=2)
    return jnp.concatenate([upper, lower], axis=1)

def split_heads(matrix, sequence_count, proposal_count, number_of_heads):
    return matrix.astype(jnp.float32).reshape(sequence_count, proposal_count, number_of_heads, -1).transpose(0, 2, 1, 3)

def delta_recursion(query_projected, key_projected, value_projected, output_gate_logits, write_strength_logits, decay_logits, decay_speed, proposal_group, head_norm_gain, state, previous_keys, previous_values, previous_log_decay, previous_strengths, accepted, parent, channel_count_total):
    sequence_count, number_of_heads, value_dim, head_dim = state.shape
    proposal_count = parent.shape[1]
    queries = unit_rows(split_heads(query_projected, sequence_count, proposal_count, number_of_heads)) * head_dim ** (-0.5)
    new_keys = unit_rows(split_heads(key_projected, sequence_count, proposal_count, number_of_heads))
    old_keys = unit_rows(split_heads(previous_keys, sequence_count, proposal_count, number_of_heads))
    new_values = split_heads(value_projected, sequence_count, proposal_count, number_of_heads)
    old_values = split_heads(previous_values, sequence_count, proposal_count, number_of_heads)
    zgate = split_heads(output_gate_logits, sequence_count, proposal_count, number_of_heads)
    beta_new = jax.nn.sigmoid(write_strength_logits.reshape(sequence_count, proposal_count, number_of_heads)).transpose(0, 2, 1)
    fresh_decay = (-decay_speed[None, None, :] * jax.nn.softplus(decay_logits.reshape(sequence_count, proposal_count, number_of_heads)) + proposal_group).transpose(0, 2, 1)
    position = jnp.arange(proposal_count, dtype=jnp.int32)
    live = (position[None, :] < accepted[:, None]).astype(jnp.float32)[:, None, :]
    beta_old = previous_strengths.transpose(0, 2, 1) * live
    decay_old = previous_log_decay.transpose(0, 2, 1) * live
    keys_all = jnp.concatenate([old_keys, new_keys], axis=2)
    values_all = jnp.concatenate([old_values, new_values], axis=2)
    beta_all = jnp.concatenate([beta_old, beta_new], axis=2)
    decay_all = jnp.concatenate([decay_old, fresh_decay], axis=2)
    visible = visibility(parent)
    gamma_sum = decay_all + exact_product('bij,bhj->bhi', visible, decay_all)
    gamma_diff = gamma_sum[:, :, :, None] - gamma_sum[:, :, None, :]
    decay_pair = jnp.exp(jnp.minimum(gamma_diff, 0.0)) * visible[:, None]
    coupling = beta_all[..., None] * exact_product('bhid,bhjd->bhij', keys_all, keys_all) * decay_pair
    right_side = jnp.concatenate([beta_all[..., None] * values_all, (beta_all * jnp.exp(gamma_sum))[..., None] * keys_all], axis=-1)
    solved = []
    for row_index in range(2 * proposal_count):
        current = right_side[:, :, row_index]
        if row_index > 0:
            current = current - exact_product('bhj,bhjd->bhd', coupling[:, :, row_index, :row_index], jnp.stack(solved, axis=2))
        solved.append(current)
    solution = jnp.stack(solved, axis=2)
    update = solution[..., :value_dim] - exact_product('bhcd,bhed->bhce', solution[..., value_dim:], state)
    identity = jnp.eye(2 * proposal_count, dtype=jnp.float32)
    seen = visible[:, proposal_count:] + identity[proposal_count:][None]
    reach = jnp.exp(jnp.minimum(gamma_diff[:, :, proposal_count:], 0.0)) * seen[:, None]
    query_key = exact_product('bhid,bhjd->bhij', queries, keys_all) * reach
    readout = exact_product('bhid,bhed->bhie', queries * jnp.exp(gamma_sum[:, :, proposal_count:])[..., None], state)
    readout = readout + exact_product('bhij,bhje->bhie', query_key, update)
    squares = channel_count_total(lax.optimization_barrier(jnp.sum(readout * readout, axis=-1)))
    readout = readout * lax.rsqrt(squares / head_dim + epsilon)[..., None]
    readout = readout * head_norm_gain.astype(jnp.float32) * jax.nn.silu(zgate)
    blended_rows = readout.transpose(0, 2, 1, 3).reshape(sequence_count * proposal_count, number_of_heads * value_dim)
    blended_rows = blended_rows.astype(jnp.bfloat16)
    last_gamma = gamma_sum[:, :, proposal_count - 1:proposal_count]
    key_weighted = old_keys * jnp.exp(last_gamma - gamma_sum[:, :, :proposal_count])[..., None]
    accepted_state = jnp.exp(last_gamma)[..., None] * state + exact_product('bhcd,bhce->bhed', key_weighted, update[:, :, :proposal_count])
    return (blended_rows, accepted_state)

def kept_channel_total(squares):
    return squares

def reference(tokens, input_norm_gain, query_weight, key_weight, value_weight, output_gate_weight, strength_weight, decay_weight, head_decay_rate, proposal_log_decay, head_norm_gain, output_weight, output_norm_gain, state, previous_keys, previous_values, previous_log_decay, previous_strengths, accepted, parent):
    sequence_count, proposal_count, width = tokens.shape
    features = tokens.astype(jnp.float32)
    normed = features * lax.rsqrt(lax.optimization_barrier(jnp.mean(features * features, axis=-1, keepdims=True)) + epsilon)
    normed = (normed * input_norm_gain.astype(jnp.float32)).astype(jnp.bfloat16)
    flat_rows = normed.reshape(sequence_count * proposal_count, width)
    query_projected = jnp.dot(flat_rows, query_weight, preferred_element_type=jnp.float32).astype(jnp.bfloat16)
    key_projected = jnp.dot(flat_rows, key_weight, preferred_element_type=jnp.float32).astype(jnp.bfloat16)
    value_projected = jnp.dot(flat_rows, value_weight.reshape(width, -1), preferred_element_type=jnp.float32).astype(jnp.bfloat16)
    output_gate_logits = jnp.dot(flat_rows, output_gate_weight.reshape(width, -1), preferred_element_type=jnp.float32).astype(jnp.bfloat16)
    write_strength_logits = jnp.dot(flat_rows, strength_weight, preferred_element_type=jnp.float32)
    decay_logits = jnp.dot(flat_rows, decay_weight, preferred_element_type=jnp.float32)
    blended_rows, accepted_state = delta_recursion(query_projected, key_projected, value_projected, output_gate_logits, write_strength_logits, decay_logits, head_decay_rate, proposal_log_decay, head_norm_gain, state, previous_keys, previous_values, previous_log_decay, previous_strengths, accepted, parent, kept_channel_total)
    combined = jnp.dot(blended_rows, output_weight.reshape(-1, width), preferred_element_type=jnp.float32)
    combined = combined * lax.rsqrt(lax.optimization_barrier(jnp.mean(combined * combined, axis=-1, keepdims=True)) + epsilon)
    layer_out = (combined * output_norm_gain.astype(jnp.float32)).astype(jnp.bfloat16).reshape(sequence_count, proposal_count, width)
    return (layer_out, accepted_state)
```

```python
import jax
import jax.numpy as jnp
from jax import lax
from jax.experimental import pallas as pl
from jax.experimental.pallas import tpu as pltpu
from jax.sharding import PartitionSpec as P

epsilon = 1e-06
f32 = jnp.float32
bf16 = jnp.bfloat16
BOTH = ("kv", "tp")


def dot(a, b, ca, cb):
    return lax.dot_general(a, b, (((ca,), (cb,)), ((), ())), preferred_element_type=f32)


def iota(shape, dim):
    return lax.broadcasted_iota(jnp.int32, shape, dim)


def roll(x, shift):
    return pltpu.roll(x, shift, 1)


def split(x):
    hi = x.astype(bf16)
    return hi, (x - hi.astype(f32)).astype(bf16)


def cost(flops, size):
    return pl.CostEstimate(flops=flops, bytes_accessed=size, transcendentals=0)


def chunk_lanes(rows, group):
    lane = iota((1, 128), 1)
    packed = None
    for j in range(4):
        if isinstance(group, int):
            half = rows[j][:, 128 * (group // 4) : 128 * (group // 4) + 128]
            shift = (32 * j - 32 * (group % 4)) % 128
            moved = roll(half, shift) if shift else half
        else:
            half = jnp.where(group >= 4, rows[j][:, 128:], rows[j][:, :128])
            moved = roll(half, lax.rem(32 * j + 128 - 32 * lax.rem(group, 4), 128))
        packed = moved if packed is None else jnp.where(lane // 32 == j, moved, packed)
    return packed


def solve(rhs, coupling):
    x = rhs
    for _ in range(3):
        x = rhs - sum(coupling[d] * roll(x, 32 * d) for d in (1, 2, 3))
    return x


def send_tokens_kernel(x_ref, out_ref):
    rows = [x_ref[i].astype(f32) for i in range(4)]
    for t in range(8):
        block = chunk_lanes(rows, t).astype(bf16)
        for k in range(16):
            out_ref[k, t] = block


def send_tokens(tokens):
    return pl.pallas_call(
        send_tokens_kernel,
        out_shape=jax.ShapeDtypeStruct((16, 8, 16, 128), bf16),
        cost_estimate=cost(1000000, 1 << 19),
        name="send_tokens",
    )(tokens)


def state_kernel(state_ref, key_ref, value_ref, strength_ref, decay_ref, accepted_ref, out_ref, low_ref):
    group = pl.program_id(0)
    lane = iota((1, 128), 1)
    place = lane // 32
    values = chunk_lanes([value_ref[j].astype(f32) for j in range(4)], group)
    strength = chunk_lanes([strength_ref[j : j + 1, :] for j in range(4)], group)
    decay = chunk_lanes([decay_ref[j : j + 1, :] for j in range(4)], group)
    accepted = chunk_lanes([accepted_ref[...]] * 4, group)
    live = jnp.where(place < accepted, 1.0, 0.0)
    beta = strength * live
    g = decay * live
    gam = g + sum(jnp.where(place >= d, roll(g, 32 * d), 0.0) for d in (1, 2, 3))
    last = g + sum(roll(g, 32 * d) for d in (1, 2, 3))
    row = iota((128, 128), 0)
    column = iota((128, 128), 1)
    order = jnp.where(column == (row % 32) * 4 + row // 32, 1.0, 0.0).astype(bf16)
    keys = dot(order, key_ref[...], 1, 0).astype(bf16)
    gram = dot(keys, keys, 1, 1)

    def diagonal(d):
        return jnp.sum(jnp.where(row == column - 32 * d, gram, 0.0), axis=0, keepdims=True)

    unit = lax.rsqrt(diagonal(0) + epsilon)
    coupling = {
        d: jnp.where(
            place >= d,
            beta * diagonal(d) * unit * roll(unit, 32 * d) * jnp.exp(jnp.minimum(gam - roll(gam, 32 * d), 0.0)),
            0.0,
        )
        for d in (1, 2, 3)
    }
    state = state_ref[...]
    flat = state.reshape(512, 128)
    high, low = split(flat)
    seen = dot(high, keys, 1, 1) + dot(low, keys, 1, 1)
    own = iota((32, 16, 128), 0) == iota((32, 16, 128), 2) % 32
    seen = jnp.sum(jnp.where(own, seen.reshape(32, 16, 128), 0.0), axis=0)
    update = solve(beta * (values - jnp.exp(gam) * unit * seen), coupling)
    update = update * (jnp.exp(last - gam) * unit)
    spread = jnp.where(own, jnp.broadcast_to(update[None], (32, 16, 128)), 0.0).reshape(512, 128)
    high, low = split(spread)
    change = dot(high, keys, 1, 0) + dot(low, keys, 1, 0)
    keep = jnp.where(iota((32, 128), 0) == iota((32, 128), 1), jnp.exp(last), 0.0)
    keep = jnp.sum(keep, axis=1, keepdims=True)
    keep = jnp.broadcast_to(jnp.broadcast_to(keep, (32, 128))[:, None, :], (32, 16, 128))
    new = keep * state + change.reshape(32, 16, 128)
    out_ref[...] = new
    low_ref[...] = new.reshape(512, 128).astype(bf16)


def new_state(state, keys, values, strengths, decays, accepted):
    return pl.pallas_call(
        state_kernel,
        grid=(8,),
        in_specs=[
            pl.BlockSpec((32, 16, 128), lambda i: (i, 0, 0)),
            pl.BlockSpec((128, 128), lambda i: (i, 0)),
            pl.BlockSpec((4, 16, 256), lambda i: (0, 0, 0)),
            pl.BlockSpec((4, 256), lambda i: (0, 0)),
            pl.BlockSpec((4, 256), lambda i: (0, 0)),
            pl.BlockSpec((1, 256), lambda i: (0, 0)),
        ],
        out_specs=[
            pl.BlockSpec((32, 16, 128), lambda i: (i, 0, 0)),
            pl.BlockSpec((512, 128), lambda i: (i, 0)),
        ],
        out_shape=[
            jax.ShapeDtypeStruct((256, 16, 128), f32),
            jax.ShapeDtypeStruct((4096, 128), bf16),
        ],
        cost_estimate=cost(2000000000, 5 << 20),
        name="new_state",
    )(state, keys, values, strengths, decays, accepted)


def rows_kernel(
    x_ref, gain_ref, wq_ref, wk_ref, scalars_ref, *rest
):
    packs, (log_decay_ref, parent_ref, rate_ref, index_ref, high_ref, low_ref, pv_ref, gate_ref) = rest[:8], rest[8:]
    group = index_ref[0, 0]
    x = x_ref[...].astype(f32)
    scale = lax.rsqrt(jnp.mean(x * x, axis=0, keepdims=True) + epsilon)
    normed = (x * scale * gain_ref[...].astype(f32)).astype(bf16)

    def project(weight, dim):
        return dot(weight, normed, dim, 0)

    def rounded(x):
        return x.astype(bf16).astype(f32)

    queries = rounded(project(wq_ref[...], 0))
    keys = rounded(project(wk_ref[...], 0))
    logits = project(scalars_ref[...], 1)
    both = jnp.concatenate(
        [pack[0:16, :2048] for pack in packs] + [pack[16:32, :2048] for pack in packs], axis=0
    )
    both = rounded(project(both, 1))
    values, zgate = both[:128], both[128:]
    gain = jnp.concatenate([pack[16:32, 2048:] for pack in packs], axis=0).astype(f32)

    def unit(x):
        return x * lax.rsqrt(jnp.sum(x * x, axis=0, keepdims=True) + epsilon)

    queries = unit(queries) * 128**-0.5
    keys = unit(keys)
    beta = jax.nn.sigmoid(logits[0:1, :])
    pre = logits[1:2, :]
    softplus = jnp.maximum(pre, 0.0) + jnp.log1p(jnp.exp(-jnp.abs(pre)))
    log_decay = chunk_lanes([log_decay_ref[i : i + 1, :] for i in range(4)], group)
    parent = chunk_lanes([parent_ref[i : i + 1, :] for i in range(4)], group)
    g = log_decay - rate_ref[0, 0] * softplus
    place = (iota((1, 128), 1) // 32).astype(f32)
    hit = {d: jnp.where((parent == place - d) & (place >= d), 1.0, 0.0) for d in (1, 2, 3)}
    seen = {1: hit[1]}
    seen[2] = hit[2] + hit[1] * roll(seen[1], 32)
    seen[3] = hit[3] + hit[1] * roll(seen[2], 32) + hit[2] * roll(seen[1], 64)
    gam = g + sum(seen[d] * roll(g, 32 * d) for d in (1, 2, 3))
    coupling, reach = {}, {0: jnp.sum(queries * keys, axis=0, keepdims=True)}
    for d in (1, 2, 3):
        earlier = roll(keys, 32 * d)
        weight = jnp.exp(jnp.minimum(gam - roll(gam, 32 * d), 0.0)) * seen[d]
        coupling[d] = beta * weight * jnp.sum(keys * earlier, axis=0, keepdims=True)
        reach[d] = weight * jnp.sum(queries * earlier, axis=0, keepdims=True)
    solved_values = solve(beta * values, coupling)
    solved_keys = solve((beta * jnp.exp(gam)) * keys, coupling)

    def reached(x):
        return reach[0] * x + sum(reach[d] * roll(x, 32 * d) for d in (1, 2, 3))

    probe = jnp.exp(gam) * queries - reached(solved_keys)
    high_ref[...], low_ref[...] = split(probe)
    pv_ref[...] = reached(solved_values)
    gate_ref[...] = gain * (zgate * jax.nn.sigmoid(zgate))


def vmem_specs(count):
    return [pl.BlockSpec(memory_space=pltpu.VMEM)] * count


def row_side(x, gain, wq, wk, scalars, packs, log_decay, parent, rate, index):
    return pl.pallas_call(
        rows_kernel,
        in_specs=vmem_specs(15) + [pl.BlockSpec(memory_space=pltpu.SMEM)] * 2,
        out_specs=vmem_specs(4),
        out_shape=[
            jax.ShapeDtypeStruct((128, 128), bf16),
            jax.ShapeDtypeStruct((128, 128), bf16),
            jax.ShapeDtypeStruct((128, 128), f32),
            jax.ShapeDtypeStruct((128, 128), f32),
        ],
        cost_estimate=cost(2000000000, 4 << 20),
        name="row_side",
    )(x, gain, wq, wk, scalars, *packs, log_decay, parent, rate, index)


def readout_kernel(state_ref, high_ref, low_ref, pv_ref, gate_ref, *rest):
    packs, (index_ref, out_ref) = rest[:8], rest[8:]
    index = index_ref[0, 0]
    own = iota((32, 16, 128), 0) == iota((32, 16, 128), 2) % 32
    pieces = []
    for d in range(8):
        block = state_ref[lax.rem(index + d, 8)]
        read = dot(block, high_ref[...], 1, 0) + dot(block, low_ref[...], 1, 0)
        pieces.append(jnp.sum(jnp.where(own, read.reshape(32, 16, 128), 0.0), axis=0))
    o = jnp.concatenate(pieces, axis=0) + pv_ref[...]
    o = o * lax.rsqrt(jnp.mean(o * o, axis=0, keepdims=True) + epsilon)
    o = (o * gate_ref[...]).astype(bf16)
    weight = jnp.concatenate([pack[32:48, :2048] for pack in packs], axis=0)
    out_ref[...] = dot(o, weight, 0, 0).astype(bf16)


def readout(state, high, low, pv, gate, packs, index):
    return pl.pallas_call(
        readout_kernel,
        in_specs=vmem_specs(13) + [pl.BlockSpec(memory_space=pltpu.SMEM)],
        out_specs=pl.BlockSpec(memory_space=pltpu.VMEM),
        out_shape=jax.ShapeDtypeStruct((128, 2048), bf16),
        cost_estimate=cost(500000000, 3 << 20),
        name="readout",
    )(state, high, low, pv, gate, *packs, index)


def total_kernel(part_ref, out_ref):
    total = jnp.sum(part_ref[...].astype(f32), axis=0)
    total = total * lax.rsqrt(jnp.mean(total * total, axis=1, keepdims=True) + epsilon)
    stacked = jnp.concatenate([total[:, 128 * c : 128 * c + 128] for c in range(16)], axis=0)
    out_ref[...] = stacked.T


def sum_heads(parts):
    return pl.pallas_call(
        total_kernel,
        in_specs=vmem_specs(1),
        out_specs=pl.BlockSpec(memory_space=pltpu.VMEM),
        out_shape=jax.ShapeDtypeStruct((128, 128), f32),
        cost_estimate=cost(1000000, 1 << 19),
        name="sum_heads",
    )(parts)


def final_kernel(x_ref, gain_ref, out_ref, scratch):
    scratch[...] = x_ref[...].T * gain_ref[...]
    lane = iota((1, 128), 1)
    rows = [scratch[pl.ds(r, 16, 8), :] for r in range(8)]
    blocks = []
    for i in range(4):
        halves = []
        for h in range(2):
            packed = None
            for q in range(4):
                shift = (32 * q - 32 * i) % 128
                moved = roll(rows[4 * h + q], shift) if shift else rows[4 * h + q]
                packed = moved if packed is None else jnp.where(lane // 32 == q, moved, packed)
            halves.append(packed)
        blocks.append(jnp.concatenate(halves, axis=1))
    full = jnp.concatenate(blocks, axis=0).astype(bf16)
    source = iota((256, 256), 0)
    target = iota((256, 256), 1)
    wanted = (source % 8) * 32 + ((source // 8) % 4) * 8 + source // 32
    order = jnp.where(wanted == target, 1.0, 0.0).astype(bf16)
    out_ref[...] = dot(full, order, 1, 0).astype(bf16).reshape(4, 16, 256)


def final_rows(x, gain):
    return pl.pallas_call(
        final_kernel,
        in_specs=vmem_specs(2),
        out_specs=pl.BlockSpec(memory_space=pltpu.VMEM),
        out_shape=jax.ShapeDtypeStruct((4, 16, 256), bf16),
        scratch_shapes=[pltpu.VMEM((128, 128), f32)],
        cost_estimate=cost(10000000, 1 << 18),
        name="final_rows",
    )(x, gain)


def on_device(
    tokens,
    input_norm_gain,
    query_weight,
    key_weight,
    value_weight,
    output_gate_weight,
    strength_weight,
    decay_weight,
    head_decay_rate,
    proposal_log_decay,
    head_norm_gain,
    output_weight,
    output_norm_gain,
    state,
    previous_keys,
    previous_values,
    previous_log_decay,
    previous_strengths,
    accepted,
    parent,
):
    tp = lax.axis_index("tp").astype(jnp.int32)
    index = tp.reshape(1, 1)

    sent = send_tokens(jnp.transpose(tokens, (1, 2, 0))).reshape(128, 16, 128)
    x = lax.all_to_all(sent, BOTH, 0, 0, tiled=True).reshape(2048, 128)

    value_rows = jnp.transpose(value_weight[:, 0, :], (1, 0))
    gate_rows = jnp.transpose(output_gate_weight[:, 0, :], (1, 0))
    output_rows = output_weight[0].reshape(16, 128, 16).transpose(0, 2, 1).reshape(16, 2048)
    gain_lanes = jnp.broadcast_to(head_norm_gain[:, None], (16, 128))
    pack = jnp.concatenate(
        [
            jnp.concatenate([value_rows, gate_rows, output_rows], axis=0),
            jnp.concatenate([gain_lanes] * 3, axis=0),
        ],
        axis=1,
    )
    packs = [pack] + [lax.ppermute(pack, "tp", [((i + d) % 8, i) for i in range(8)]) for d in range(1, 8)]

    old_values = jnp.transpose(previous_values[:, :, 0, :], (1, 2, 0))
    accepted_state, low_state = new_state(
        state.reshape(256, 16, 128),
        previous_keys.reshape(1024, 128),
        old_values,
        jnp.transpose(previous_strengths[:, :, 0], (1, 0)),
        jnp.transpose(previous_log_decay[:, :, 0], (1, 0)),
        accepted.astype(f32).reshape(1, 256),
    )
    moved_state = lax.all_to_all(low_state.reshape(8, 512, 128), "tp", 0, 0, tiled=True)

    scalars = jnp.concatenate(
        [jnp.transpose(strength_weight, (1, 0)), jnp.transpose(decay_weight, (1, 0)), jnp.zeros((14, 2048), bf16)], axis=0
    )
    high, low, pv, gate = row_side(
        x,
        jnp.broadcast_to(input_norm_gain[:, None], (2048, 128)),
        query_weight,
        key_weight,
        scalars,
        packs,
        jnp.transpose(proposal_log_decay[:, :, 0], (1, 0)),
        jnp.transpose(parent, (1, 0)).astype(f32),
        head_decay_rate.reshape(1, 1),
        index,
    )
    part = readout(moved_state, high, low, pv, gate, packs, index)
    parts = lax.all_to_all(part.reshape(16, 8, 2048), "kv", 0, 0, tiled=True)
    blocks = lax.all_to_all(sum_heads(parts), BOTH, 0, 0, tiled=True)
    gain_rows = jnp.broadcast_to(jnp.repeat(output_norm_gain.astype(f32), 8)[:, None], (128, 128))
    out = final_rows(blocks, gain_rows)
    return jnp.transpose(out, (2, 0, 1)), accepted_state.reshape(state.shape)


def solution(mesh):
    placed = (
        P(None, None, ("kv", "tp")),
        P(),
        P(None, "kv"),
        P(None, "kv"),
        P(None, "kv", "tp"),
        P(None, "kv", "tp"),
        P(None, "kv"),
        P(None, "kv"),
        P("kv"),
        P(None, None, "kv"),
        P("tp"),
        P("kv", "tp", None),
        P(("kv", "tp")),
        P(None, "kv", "tp", None),
        P(None, None, "kv"),
        P(None, None, "kv", "tp"),
        P(None, None, "kv"),
        P(None, None, "kv"),
        P(),
        P(),
    )
    return jax.shard_map(
        on_device,
        mesh=mesh,
        in_specs=placed,
        out_specs=(P(None, None, ("kv", "tp")), P(None, "kv", "tp", None)),
        check_vma=False,
    )
```

```python
import jax
import jax.numpy as jnp
from jax import lax
from jax.experimental import pallas as pl
from jax.experimental.pallas import tpu as pltpu
from jax.sharding import PartitionSpec as P


epsilon = 1e-06
f32 = jnp.float32
bf16 = jnp.bfloat16
BOTH = ("kv", "tp")
GROUPS = 2
VMEM_LIMIT = 16 << 20


def dot(a, b, ca, cb):
    return lax.dot_general(a, b, (((ca,), (cb,)), ((), ())), preferred_element_type=f32)


def iota(shape, dim):
    return lax.broadcasted_iota(jnp.int32, shape, dim)


def roll(x, shift):
    return pltpu.roll(x, shift, 1)


def split(x):
    hi = x.astype(bf16)
    return hi, (x - hi.astype(f32)).astype(bf16)


def cost(flops, size):
    return pl.CostEstimate(flops=flops, bytes_accessed=size, transcendentals=0)


def chunk_lanes(rows, group):
    lane = iota((1, 128), 1)
    packed = None
    for j in range(4):
        if isinstance(group, int):
            half = rows[j][:, 128 * (group // 4) : 128 * (group // 4) + 128]
            shift = (32 * j - 32 * (group % 4)) % 128
            moved = roll(half, shift) if shift else half
        else:
            half = jnp.where(group >= 4, rows[j][:, 128:], rows[j][:, :128])
            moved = roll(half, lax.rem(32 * j + 128 - 32 * lax.rem(group, 4), 128))
        packed = moved if packed is None else jnp.where(lane // 32 == j, moved, packed)
    return packed


def solve(rhs, coupling):
    x = rhs
    for _ in range(3):
        x = rhs - sum(coupling[d] * roll(x, 32 * d) for d in (1, 2, 3))
    return x


def send_tokens_kernel(x_ref, out_ref):
    rows = [x_ref[i].astype(f32) for i in range(4)]
    for t in range(8):
        block = chunk_lanes(rows, t).astype(bf16)
        for k in range(16):
            out_ref[k, t] = block


def send_tokens(tokens):
    return pl.pallas_call(
        send_tokens_kernel,
        out_shape=jax.ShapeDtypeStruct((16, 8, 16, 128), bf16),
        cost_estimate=cost(1000000, 1 << 19),
        compiler_params=pltpu.CompilerParams(vmem_limit_bytes=VMEM_LIMIT),
        name="send_tokens",
    )(tokens)


def state_kernel(state_ref, key_ref, value_ref, strength_ref, decay_ref, accepted_ref, out_ref, low_ref):
    for part in range(GROUPS):
        rows = pl.ds(32 * part, 32)
        new = state_of_group(
            GROUPS * pl.program_id(0) + part,
            state_ref[rows],
            key_ref[pl.ds(128 * part, 128), :],
            value_ref,
            strength_ref,
            decay_ref,
            accepted_ref,
        )
        out_ref[rows] = new
        low_ref[pl.ds(512 * part, 512), :] = new.reshape(512, 128).astype(bf16)


def state_of_group(group, state, key_rows, value_ref, strength_ref, decay_ref, accepted_ref):
    lane = iota((1, 128), 1)
    place = lane // 32
    values = chunk_lanes([value_ref[j].astype(f32) for j in range(4)], group)
    strength = chunk_lanes([strength_ref[j] for j in range(4)], group)
    decay = chunk_lanes([decay_ref[j] for j in range(4)], group)
    accepted = chunk_lanes([accepted_ref[...].astype(f32)] * 4, group)
    live = jnp.where(place < accepted, 1.0, 0.0)
    beta = strength * live
    g = decay * live
    gam = g + sum(jnp.where(place >= d, roll(g, 32 * d), 0.0) for d in (1, 2, 3))
    last = g + sum(roll(g, 32 * d) for d in (1, 2, 3))
    row = iota((128, 128), 0)
    column = iota((128, 128), 1)
    order = jnp.where(column == (row % 32) * 4 + row // 32, 1.0, 0.0).astype(bf16)
    keys = dot(order, key_rows, 1, 0).astype(bf16)
    gram = dot(keys, keys, 1, 1)

    def diagonal(d):
        return jnp.sum(jnp.where(row == column - 32 * d, gram, 0.0), axis=0, keepdims=True)

    unit = lax.rsqrt(diagonal(0) + epsilon)
    coupling = {
        d: jnp.where(
            place >= d,
            beta * diagonal(d) * unit * roll(unit, 32 * d) * jnp.exp(jnp.minimum(gam - roll(gam, 32 * d), 0.0)),
            0.0,
        )
        for d in (1, 2, 3)
    }
    flat = state.reshape(512, 128)
    high, low = split(flat)
    seen = dot(high, keys, 1, 1) + dot(low, keys, 1, 1)
    own = iota((32, 16, 128), 0) == iota((32, 16, 128), 2) % 32
    seen = jnp.sum(jnp.where(own, seen.reshape(32, 16, 128), 0.0), axis=0)
    update = solve(beta * (values - jnp.exp(gam) * unit * seen), coupling)
    update = update * (jnp.exp(last - gam) * unit)
    spread = jnp.where(own, jnp.broadcast_to(update[None], (32, 16, 128)), 0.0).reshape(512, 128)
    high, low = split(spread)
    change = dot(high, keys, 1, 0) + dot(low, keys, 1, 0)
    keep = jnp.where(iota((32, 128), 0) == iota((32, 128), 1), jnp.exp(last), 0.0)
    keep = jnp.sum(keep, axis=1, keepdims=True)
    keep = jnp.broadcast_to(jnp.broadcast_to(keep, (32, 128))[:, None, :], (32, 16, 128))
    return keep * state + change.reshape(32, 16, 128)


def new_state(state, keys, values, strengths, decays, accepted):
    return pl.pallas_call(
        state_kernel,
        grid=(8 // GROUPS,),
        in_specs=[
            pl.BlockSpec((32 * GROUPS, 16, 128), lambda i: (i, 0, 0)),
            pl.BlockSpec((128 * GROUPS, 128), lambda i: (i, 0)),
            pl.BlockSpec((4, 16, 256), lambda i: (0, 0, 0)),
            pl.BlockSpec((4, 1, 256), lambda i: (0, 0, 0)),
            pl.BlockSpec((4, 1, 256), lambda i: (0, 0, 0)),
            pl.BlockSpec((1, 256), lambda i: (0, 0)),
        ],
        out_specs=[
            pl.BlockSpec((32 * GROUPS, 16, 128), lambda i: (i, 0, 0)),
            pl.BlockSpec((512 * GROUPS, 128), lambda i: (i, 0)),
        ],
        out_shape=[
            jax.ShapeDtypeStruct((256, 16, 128), f32),
            jax.ShapeDtypeStruct((4096, 128), bf16),
        ],
        cost_estimate=cost(2000000000, 5 << 20),
        compiler_params=pltpu.CompilerParams(vmem_limit_bytes=VMEM_LIMIT),
        name="new_state",
    )(state, keys, values, strengths, decays, accepted)


def rows_kernel(
    x_ref, gain_ref, wq_ref, wk_ref, scalars_ref, *rest
):
    packs, (log_decay_ref, parent_ref, rate_ref, index_ref, high_ref, low_ref, pv_ref, gate_ref) = rest[:8], rest[8:]
    group = index_ref[0, 0]
    x = x_ref[...].astype(f32)
    scale = lax.rsqrt(jnp.mean(x * x, axis=0, keepdims=True) + epsilon)
    normed = (x * scale * gain_ref[...].astype(f32)).astype(bf16)

    def project(weight, dim):
        return dot(weight, normed, dim, 0)

    def rounded(x):
        return x.astype(bf16).astype(f32)

    queries = rounded(project(wq_ref[...], 0))
    keys = rounded(project(wk_ref[...], 0))
    logits = project(scalars_ref[...], 1)
    both = jnp.concatenate(
        [pack[0:16, :2048] for pack in packs] + [pack[16:32, :2048] for pack in packs], axis=0
    )
    both = rounded(project(both, 1))
    values, zgate = both[:128], both[128:]
    gain = jnp.concatenate([pack[16:32, 2048:] for pack in packs], axis=0).astype(f32)

    def unit(x):
        return x * lax.rsqrt(jnp.sum(x * x, axis=0, keepdims=True) + epsilon)

    queries = unit(queries) * 128**-0.5
    keys = unit(keys)
    beta = jax.nn.sigmoid(logits[0:1, :])
    pre = logits[1:2, :]
    softplus = jnp.maximum(pre, 0.0) + jnp.log1p(jnp.exp(-jnp.abs(pre)))
    log_decay = chunk_lanes([log_decay_ref[i] for i in range(4)], group)
    parent = chunk_lanes([parent_ref[i : i + 1, :].astype(f32) for i in range(4)], group)
    g = log_decay - rate_ref[0, 0] * softplus
    place = (iota((1, 128), 1) // 32).astype(f32)
    hit = {d: jnp.where((parent == place - d) & (place >= d), 1.0, 0.0) for d in (1, 2, 3)}
    seen = {1: hit[1]}
    seen[2] = hit[2] + hit[1] * roll(seen[1], 32)
    seen[3] = hit[3] + hit[1] * roll(seen[2], 32) + hit[2] * roll(seen[1], 64)
    gam = g + sum(seen[d] * roll(g, 32 * d) for d in (1, 2, 3))
    coupling, reach = {}, {0: jnp.sum(queries * keys, axis=0, keepdims=True)}
    for d in (1, 2, 3):
        earlier = roll(keys, 32 * d)
        weight = jnp.exp(jnp.minimum(gam - roll(gam, 32 * d), 0.0)) * seen[d]
        coupling[d] = beta * weight * jnp.sum(keys * earlier, axis=0, keepdims=True)
        reach[d] = weight * jnp.sum(queries * earlier, axis=0, keepdims=True)
    solved_values = solve(beta * values, coupling)
    solved_keys = solve((beta * jnp.exp(gam)) * keys, coupling)

    def reached(x):
        return reach[0] * x + sum(reach[d] * roll(x, 32 * d) for d in (1, 2, 3))

    probe = jnp.exp(gam) * queries - reached(solved_keys)
    high_ref[...], low_ref[...] = split(probe)
    pv_ref[...] = reached(solved_values)
    gate_ref[...] = gain * (zgate * jax.nn.sigmoid(zgate))


def vmem_specs(count):
    return [pl.BlockSpec(memory_space=pltpu.VMEM)] * count


def row_side(x, gain, wq, wk, scalars, packs, log_decay, parent, rate, index):
    return pl.pallas_call(
        rows_kernel,
        in_specs=vmem_specs(15) + [pl.BlockSpec(memory_space=pltpu.SMEM)] * 2,
        out_specs=vmem_specs(4),
        out_shape=[
            jax.ShapeDtypeStruct((128, 128), bf16),
            jax.ShapeDtypeStruct((128, 128), bf16),
            jax.ShapeDtypeStruct((128, 128), f32),
            jax.ShapeDtypeStruct((128, 128), f32),
        ],
        cost_estimate=cost(2000000000, 4 << 20),
        compiler_params=pltpu.CompilerParams(vmem_limit_bytes=VMEM_LIMIT),
        name="row_side",
    )(x, gain, wq, wk, scalars, *packs, log_decay, parent, rate, index)


def readout_kernel(state_ref, high_ref, low_ref, pv_ref, gate_ref, *rest):
    packs, (index_ref, out_ref) = rest[:8], rest[8:]
    index = index_ref[0, 0]
    own = iota((32, 16, 128), 0) == iota((32, 16, 128), 2) % 32
    pieces = []
    chip, core = index // 2, lax.rem(index, 2)
    for d in range(8):
        block = state_ref[2 * lax.rem(chip + d % 4, 4) + (core if d < 4 else 1 - core)]
        read = dot(block, high_ref[...], 1, 0) + dot(block, low_ref[...], 1, 0)
        pieces.append(jnp.sum(jnp.where(own, read.reshape(32, 16, 128), 0.0), axis=0))
    o = jnp.concatenate(pieces, axis=0) + pv_ref[...]
    o = o * lax.rsqrt(jnp.mean(o * o, axis=0, keepdims=True) + epsilon)
    o = (o * gate_ref[...]).astype(bf16)
    weight = jnp.concatenate([pack[32:48, :2048] for pack in packs], axis=0)
    out_ref[...] = dot(o, weight, 0, 0).astype(bf16)


def readout(state, high, low, pv, gate, packs, index):
    return pl.pallas_call(
        readout_kernel,
        in_specs=vmem_specs(13) + [pl.BlockSpec(memory_space=pltpu.SMEM)],
        out_specs=pl.BlockSpec(memory_space=pltpu.VMEM),
        out_shape=jax.ShapeDtypeStruct((128, 2048), bf16),
        cost_estimate=cost(500000000, 3 << 20),
        compiler_params=pltpu.CompilerParams(vmem_limit_bytes=VMEM_LIMIT),
        name="readout",
    )(state, high, low, pv, gate, *packs, index)


def total_kernel(part_ref, out_ref):
    total = jnp.sum(part_ref[...].astype(f32), axis=0)
    total = total * lax.rsqrt(jnp.mean(total * total, axis=1, keepdims=True) + epsilon)
    stacked = jnp.concatenate([total[:, 128 * c : 128 * c + 128] for c in range(16)], axis=0)
    out_ref[...] = stacked.T


def sum_heads(parts):
    return pl.pallas_call(
        total_kernel,
        in_specs=vmem_specs(1),
        out_specs=pl.BlockSpec(memory_space=pltpu.VMEM),
        out_shape=jax.ShapeDtypeStruct((128, 128), f32),
        cost_estimate=cost(1000000, 1 << 19),
        compiler_params=pltpu.CompilerParams(vmem_limit_bytes=VMEM_LIMIT),
        name="sum_heads",
    )(parts)


def final_kernel(x_ref, gain_ref, out_ref, scratch):
    scratch[...] = x_ref[...].T * gain_ref[...]
    lane = iota((1, 128), 1)
    rows = [scratch[pl.ds(r, 16, 8), :] for r in range(8)]
    blocks = []
    for i in range(4):
        halves = []
        for h in range(2):
            packed = None
            for q in range(4):
                shift = (32 * q - 32 * i) % 128
                moved = roll(rows[4 * h + q], shift) if shift else rows[4 * h + q]
                packed = moved if packed is None else jnp.where(lane // 32 == q, moved, packed)
            halves.append(packed)
        blocks.append(jnp.concatenate(halves, axis=1))
    full = jnp.concatenate(blocks, axis=0).astype(bf16)
    source = iota((256, 256), 0)
    target = iota((256, 256), 1)
    wanted = (source % 8) * 32 + ((source // 8) % 4) * 8 + source // 32
    order = jnp.where(wanted == target, 1.0, 0.0).astype(bf16)
    out_ref[...] = dot(full, order, 1, 0).astype(bf16).reshape(4, 16, 256)


def final_rows(x, gain):
    return pl.pallas_call(
        final_kernel,
        in_specs=vmem_specs(2),
        out_specs=pl.BlockSpec(memory_space=pltpu.VMEM),
        out_shape=jax.ShapeDtypeStruct((4, 16, 256), bf16),
        scratch_shapes=[pltpu.VMEM((128, 128), f32)],
        cost_estimate=cost(10000000, 1 << 18),
        compiler_params=pltpu.CompilerParams(vmem_limit_bytes=VMEM_LIMIT),
        name="final_rows",
    )(x, gain)


def chips(x):
    return [lax.ppermute(x, "tp", [((i + 2 * d) % 8, i) for i in range(8)]) for d in range(1, 4)]


def cores(arrays):
    return [lax.ppermute(x, "tp", [(i ^ 1, i) for i in range(8)]) for x in arrays]


def whole_step(
    tokens,
    input_norm_gain,
    query_weight,
    key_weight,
    value_weight,
    output_gate_weight,
    strength_weight,
    decay_weight,
    head_decay_rate,
    proposal_log_decay,
    head_norm_gain,
    output_weight,
    output_norm_gain,
    state,
    previous_keys,
    previous_values,
    previous_log_decay,
    previous_strengths,
    accepted,
    parent,
):
    tp = lax.axis_index("tp").astype(jnp.int32)
    index = tp.reshape(1, 1)

    sent = send_tokens(jnp.transpose(tokens, (1, 2, 0))).reshape(128, 16, 128)
    x = lax.all_to_all(sent, BOTH, 0, 0, tiled=True).reshape(2048, 128)

    value_rows = jnp.transpose(value_weight[:, 0, :], (1, 0))
    gate_rows = jnp.transpose(output_gate_weight[:, 0, :], (1, 0))
    gain_lanes = jnp.broadcast_to(head_norm_gain[:, None], (16, 128))
    output_rows = output_weight[0].reshape(16, 128, 16).transpose(0, 2, 1).reshape(16, 2048)
    pack = jnp.concatenate(
        [
            jnp.concatenate([value_rows, gate_rows, output_rows], axis=0),
            jnp.concatenate([gain_lanes] * 3, axis=0),
        ],
        axis=1,
    )
    near = [pack] + chips(pack)
    packs = near + cores(near)

    old_values = jnp.transpose(previous_values[:, :, 0, :], (1, 2, 0))
    accepted_state, low_state = new_state(
        state.reshape(256, 16, 128),
        previous_keys.reshape(1024, 128),
        old_values,
        jnp.transpose(previous_strengths, (1, 2, 0)),
        jnp.transpose(previous_log_decay, (1, 2, 0)),
        accepted.reshape(1, 256),
    )
    moved_state = lax.all_to_all(low_state.reshape(8, 512, 128), "tp", 0, 0, tiled=True)

    scalars = jnp.concatenate(
        [jnp.transpose(strength_weight, (1, 0)), jnp.transpose(decay_weight, (1, 0)), jnp.zeros((14, 2048), bf16)], axis=0
    )
    high, low, pv, gate = row_side(
        x,
        jnp.broadcast_to(input_norm_gain[:, None], (2048, 128)),
        query_weight,
        key_weight,
        scalars,
        packs,
        jnp.transpose(proposal_log_decay, (1, 2, 0)),
        jnp.transpose(parent, (1, 0)),
        head_decay_rate.reshape(1, 1),
        index,
    )
    part = readout(moved_state, high, low, pv, gate, packs, index)
    parts = lax.all_to_all(part.reshape(16, 8, 2048), "kv", 0, 0, tiled=True)
    blocks = lax.all_to_all(sum_heads(parts), BOTH, 0, 0, tiled=True)
    gain_rows = jnp.broadcast_to(jnp.repeat(output_norm_gain.astype(f32), 8)[:, None], (128, 128))
    out = final_rows(blocks, gain_rows)
    return jnp.transpose(out, (2, 0, 1)), accepted_state.reshape(state.shape)


def solution(mesh):
    placed = (
        P(None, None, ("kv", "tp")),
        P(),
        P(None, "kv"),
        P(None, "kv"),
        P(None, "kv", "tp"),
        P(None, "kv", "tp"),
        P(None, "kv"),
        P(None, "kv"),
        P("kv"),
        P(None, None, "kv"),
        P("tp"),
        P("kv", "tp", None),
        P(("kv", "tp")),
        P(None, "kv", "tp", None),
        P(None, None, "kv"),
        P(None, None, "kv", "tp"),
        P(None, None, "kv"),
        P(None, None, "kv"),
        P(),
        P(),
    )
    return jax.shard_map(
        whole_step,
        mesh=mesh,
        in_specs=placed,
        out_specs=(P(None, None, ("kv", "tp")), P(None, "kv", "tp", None)),
        check_vma=False,
    )
```

```python
import jax
import jax.numpy as jnp
from jax import lax
from jax.experimental import pallas as pl
from jax.experimental.pallas import tpu as pltpu
from jax.sharding import PartitionSpec as P


epsilon = 1e-06
f32 = jnp.float32
bf16 = jnp.bfloat16
BOTH = ("kv", "tp")
VMEM_LIMIT = 16 << 20
PACK = 784


def dot(a, b, ca, cb):
    return lax.dot_general(a, b, (((ca,), (cb,)), ((), ())), preferred_element_type=f32)


def iota(shape, dim):
    return lax.broadcasted_iota(jnp.int32, shape, dim)


def roll(x, shift):
    return pltpu.roll(x, shift, 1)


def split(x):
    hi = x.astype(bf16)
    return hi, (x - hi.astype(f32)).astype(bf16)


def cost(flops, size):
    return pl.CostEstimate(flops=flops, bytes_accessed=size, transcendentals=0)


def chunk_lanes(rows, group):
    lane = iota((1, 128), 1)
    packed = None
    for j in range(4):
        if isinstance(group, int):
            half = rows[j][:, 128 * (group // 4) : 128 * (group // 4) + 128]
            shift = (32 * j - 32 * (group % 4)) % 128
            moved = roll(half, shift) if shift else half
        else:
            half = jnp.where(group >= 4, rows[j][:, 128:], rows[j][:, :128])
            moved = roll(half, lax.rem(32 * j + 128 - 32 * lax.rem(group, 4), 128))
        packed = moved if packed is None else jnp.where(lane // 32 == j, moved, packed)
    return packed


def solve(rhs, coupling):
    x = rhs
    for _ in range(3):
        x = rhs - sum(coupling[d] * roll(x, 32 * d) for d in (1, 2, 3))
    return x


def hbm_specs(count):
    return [pl.BlockSpec(memory_space=pltpu.HBM)] * count


def vmem_specs(count):
    return [pl.BlockSpec(memory_space=pltpu.VMEM)] * count


def start_all(copies):
    for copy in copies:
        copy.start()


def wait_all(copies):
    for copy in copies:
        copy.wait()


def copies_in(sources, targets, sems):
    return [pltpu.make_async_copy(x, y, sems.at[i]) for i, (x, y) in enumerate(zip(sources, targets))]


def in_hbm(arrays):
    return [pltpu.with_memory_space_constraint(x, pltpu.HBM) for x in arrays]


def scratch_like(arrays):
    return [pltpu.VMEM(x.shape, x.dtype) for x in arrays] + [pltpu.SemaphoreType.DMA((len(arrays),))]


def prepare_kernel(*refs):
    sources, (sent_ref, pack_ref), held, sems = refs[:5], refs[5:7], refs[7:12], refs[12]
    copies = copies_in(sources, held, sems)
    start_all(copies)
    wait_all(copies[1:])
    pack_weights(*held[1:], pack_ref)
    copies[0].wait()
    rows = [held[0][i].astype(f32) for i in range(4)]
    for t in range(8):
        block = chunk_lanes(rows, t).astype(bf16)
        for k in range(16):
            sent_ref[k, t] = block


def prepare(*arrays):
    return pl.pallas_call(
        prepare_kernel,
        in_specs=hbm_specs(5),
        out_specs=vmem_specs(2),
        out_shape=[pltpu.VMEM((16, 8, 16, 128), bf16), pltpu.VMEM((PACK, 128), bf16)],
        scratch_shapes=scratch_like(arrays),
        cost_estimate=cost(10000000, 1 << 20),
        compiler_params=pltpu.CompilerParams(vmem_limit_bytes=VMEM_LIMIT),
        name="prepare",
    )(*in_hbm(arrays))


def stack(rows):
    return jnp.concatenate(rows, axis=0)


def spread_rows(x):
    return jnp.broadcast_to(x[:, None, :], (8, 16, 128)).reshape(128, 128)


def state_kernel(*refs):
    state_source, sources, state_out, lows, state_ref, held, (sems, state_sems) = (
        refs[0], refs[1:6], refs[6], refs[7:11], refs[11], refs[12:17], refs[17:],
    )
    key_ref, value_ref, strength_ref, decay_ref, accepted_ref = held
    chip = lax.axis_index("tp") // 2
    groups = [2 * lax.rem(chip + step // 2, 4) + step % 2 for step in range(8)]

    def rows_of(step, count=1):
        return pl.ds(pl.multiple_of(32 * groups[step], 32), 32 * count)

    copies = copies_in(sources, held, sems)
    loads = [
        pltpu.make_async_copy(state_source.at[rows_of(2 * i, 2)], state_ref.at[rows_of(2 * i, 2)], state_sems.at[0, i])
        for i in range(4)
    ]
    stores = [
        pltpu.make_async_copy(state_ref.at[rows_of(2 * i, 2)], state_out.at[rows_of(2 * i, 2)], state_sems.at[1, i])
        for i in range(4)
    ]
    start_all(copies + loads)
    wait_all(copies)

    lane = iota((1, 128), 1)
    place = lane // 32
    strength = stack([chunk_lanes([strength_ref[j] for j in range(4)], x) for x in groups])
    decay = stack([chunk_lanes([decay_ref[j] for j in range(4)], x) for x in groups])
    accepted = stack([chunk_lanes([accepted_ref[...].astype(f32)] * 4, x) for x in groups])
    values = [value_ref[j].astype(f32) for j in range(4)]
    values = stack([chunk_lanes(values, x) for x in groups])
    live = jnp.where(place < accepted, 1.0, 0.0)
    beta = strength * live
    g = decay * live
    gam = g + sum(jnp.where(place >= d, roll(g, 32 * d), 0.0) for d in (1, 2, 3))
    last = g + sum(roll(g, 32 * d) for d in (1, 2, 3))
    row = iota((128, 128), 0)
    column = iota((128, 128), 1)
    order = jnp.where(column == (row % 32) * 4 + row // 32, 1.0, 0.0).astype(bf16)
    keys = [dot(order, key_ref[pl.ds(pl.multiple_of(128 * x, 128), 128), :], 1, 0).astype(bf16) for x in groups]
    grams = [dot(x, x, 1, 1) for x in keys]

    def diagonal(d):
        return stack(
            [jnp.sum(jnp.where(row == column - 32 * d, gram, 0.0), axis=0, keepdims=True) for gram in grams]
        )

    unit = lax.rsqrt(diagonal(0) + epsilon)
    coupling = {
        d: jnp.where(
            place >= d,
            beta * diagonal(d) * unit * roll(unit, 32 * d) * jnp.exp(jnp.minimum(gam - roll(gam, 32 * d), 0.0)),
            0.0,
        )
        for d in (1, 2, 3)
    }
    coupling = {d: spread_rows(x) for d, x in coupling.items()}
    own = iota((32, 16, 128), 0) == iota((32, 16, 128), 2) % 32
    seen = []
    for step in range(8):
        if step % 2 == 0:
            loads[step // 2].wait()
        high, low = split(state_ref[rows_of(step)].reshape(512, 128))
        read = dot(high, keys[step], 1, 1) + dot(low, keys[step], 1, 1)
        seen.append(jnp.sum(jnp.where(own, read.reshape(32, 16, 128), 0.0), axis=0))
    update = solve(spread_rows(beta) * values - spread_rows(beta * jnp.exp(gam) * unit) * stack(seen), coupling)
    update = update * spread_rows(jnp.exp(last - gam) * unit)
    keep = jnp.exp(last)
    for step in range(8):
        spread = jnp.broadcast_to(update[16 * step : 16 * step + 16][None], (32, 16, 128))
        high, low = split(jnp.where(own, spread, 0.0).reshape(512, 128))
        change = dot(high, keys[step], 1, 0) + dot(low, keys[step], 1, 0)
        kept = jnp.where(iota((32, 128), 0) == iota((32, 128), 1), keep[step : step + 1], 0.0)
        kept = jnp.broadcast_to(jnp.sum(kept, axis=1, keepdims=True), (32, 128))
        kept = jnp.broadcast_to(kept[:, None, :], (32, 16, 128))
        new = kept * state_ref[rows_of(step)] + change.reshape(32, 16, 128)
        state_ref[rows_of(step)] = new
        lows[step // 2][512 * (step % 2) : 512 * (step % 2) + 512, :] = new.reshape(512, 128).astype(bf16)
        if step % 2 == 1:
            stores[step // 2].start()
    wait_all(stores)


def new_state(state, *arrays):
    return pl.pallas_call(
        state_kernel,
        in_specs=hbm_specs(6),
        out_specs=hbm_specs(1) + vmem_specs(4),
        out_shape=[pltpu.HBM((256, 16, 128), f32)] + [pltpu.VMEM((1024, 128), bf16)] * 4,
        scratch_shapes=[pltpu.VMEM((256, 16, 128), f32), *scratch_like(arrays), pltpu.SemaphoreType.DMA((2, 4))],
        cost_estimate=cost(2000000000, 5 << 20),
        compiler_params=pltpu.CompilerParams(vmem_limit_bytes=VMEM_LIMIT),
        name="new_state",
    )(*in_hbm((state, *arrays)))


def pack_weights(value_ref, gate_ref, output_ref, gain_ref, pack_ref):
    row = iota((16, 16), 0)
    gain = jnp.where(row == iota((16, 16), 1), jnp.broadcast_to(gain_ref[...].astype(f32), (16, 16)), 0.0)
    gain = jnp.broadcast_to(jnp.sum(gain, axis=1, keepdims=True), (16, 128)).astype(bf16)
    source = iota((128, 128), 0)
    target = iota((128, 128), 1)
    order = jnp.where(target == (source % 16) * 8 + source // 16, 1.0, 0.0).astype(bf16)
    rows = jnp.concatenate([output_ref[:, 128 * b : 128 * b + 128] for b in range(16)], axis=0)
    rows = dot(rows, order, 1, 0)
    lane = iota((1, 128), 1)
    for c in range(16):
        packed = None
        for b in range(16):
            piece = rows[16 * b : 16 * b + 16, :]
            shift = (8 * (b - c)) % 128
            moved = roll(piece, shift) if shift else piece
            packed = moved if packed is None else jnp.where(lane // 8 == b, moved, packed)
        columns = slice(128 * c, 128 * c + 128)
        block = jnp.concatenate([value_ref[:, columns], gate_ref[:, columns], packed.astype(bf16)], axis=0)
        pack_ref[48 * c : 48 * c + 48, :] = block
    pack_ref[768:, :] = gain


def weight_rows(packs, first):
    return jnp.concatenate(
        [
            jnp.concatenate([x[48 * b + first : 48 * b + first + 16, :] for x in packs], axis=0)
            for b in range(16)
        ],
        axis=1,
    )


def rows_kernel(x_ref, *refs):
    packs, rate_ref, sources, rest = refs[:8], refs[8], refs[9:16], refs[16:]
    (high_ref, low_ref, pv_ref, gate_ref), held, sems = rest[:4], rest[4:11], rest[11]
    gain_ref, wq_ref, wk_ref, strength_ref, decay_ref, log_decay_ref, parent_ref = held
    copies = copies_in(sources, held, sems)
    start_all(copies)
    wait_all(copies)
    group = lax.axis_index("tp")
    x = x_ref[...].astype(f32)
    scale = lax.rsqrt(jnp.mean(x * x, axis=0, keepdims=True) + epsilon)
    column = iota((128, 128), 1) == iota((128, 128), 0)
    gain = jnp.concatenate(
        [jnp.where(column, gain_ref[b : b + 1, :].astype(f32), 0.0).astype(bf16) for b in range(16)], axis=0
    )
    gain = dot(gain, jnp.ones((128, 128), bf16), 1, 0)
    normed = (x * scale * gain).astype(bf16)

    def project(weight, dim):
        return dot(weight, normed, dim, 0)

    def rounded(x):
        return x.astype(bf16).astype(f32)

    queries = rounded(project(wq_ref[...], 0))
    keys = rounded(project(wk_ref[...], 0))
    first = iota((16, 2048), 0) == 0
    scalars = jnp.where(first, strength_ref[...].astype(f32), decay_ref[...].astype(f32))
    logits = project(scalars.astype(bf16), 1)
    both = jnp.concatenate([weight_rows(packs, 0), weight_rows(packs, 16)], axis=0)
    both = rounded(project(both, 1))
    values, zgate = both[:128], both[128:]
    gain = jnp.concatenate([pack[768:, :] for pack in packs], axis=0).astype(f32)

    def unit(x):
        return x * lax.rsqrt(jnp.sum(x * x, axis=0, keepdims=True) + epsilon)

    queries = unit(queries) * 128**-0.5
    keys = unit(keys)
    beta = jax.nn.sigmoid(logits[0:1, :])
    pre = logits[1:2, :]
    softplus = jnp.maximum(pre, 0.0) + jnp.log1p(jnp.exp(-jnp.abs(pre)))
    log_decay = chunk_lanes([log_decay_ref[i] for i in range(4)], group)
    parent = chunk_lanes([parent_ref[i : i + 1, :].astype(f32) for i in range(4)], group)
    g = log_decay - rate_ref[0, 0] * softplus
    place = (iota((1, 128), 1) // 32).astype(f32)
    hit = {d: jnp.where((parent == place - d) & (place >= d), 1.0, 0.0) for d in (1, 2, 3)}
    seen = {1: hit[1]}
    seen[2] = hit[2] + hit[1] * roll(seen[1], 32)
    seen[3] = hit[3] + hit[1] * roll(seen[2], 32) + hit[2] * roll(seen[1], 64)
    gam = g + sum(seen[d] * roll(g, 32 * d) for d in (1, 2, 3))
    coupling, reach = {}, {0: jnp.sum(queries * keys, axis=0, keepdims=True)}
    for d in (1, 2, 3):
        earlier = roll(keys, 32 * d)
        weight = jnp.exp(jnp.minimum(gam - roll(gam, 32 * d), 0.0)) * seen[d]
        coupling[d] = beta * weight * jnp.sum(keys * earlier, axis=0, keepdims=True)
        reach[d] = weight * jnp.sum(queries * earlier, axis=0, keepdims=True)
    solved_values = solve(beta * values, coupling)
    solved_keys = solve((beta * jnp.exp(gam)) * keys, coupling)

    def reached(x):
        return reach[0] * x + sum(reach[d] * roll(x, 32 * d) for d in (1, 2, 3))

    probe = jnp.exp(gam) * queries - reached(solved_keys)
    high_ref[...], low_ref[...] = split(probe)
    pv_ref[...] = reached(solved_values)
    gate_ref[...] = gain * (zgate * jax.nn.sigmoid(zgate))


def row_side(x, packs, rate, *arrays):
    return pl.pallas_call(
        rows_kernel,
        in_specs=vmem_specs(9) + [pl.BlockSpec(memory_space=pltpu.SMEM)] + hbm_specs(7),
        out_specs=vmem_specs(4),
        out_shape=[
            pltpu.VMEM((128, 128), bf16),
            pltpu.VMEM((128, 128), bf16),
            pltpu.VMEM((128, 128), f32),
            pltpu.VMEM((128, 128), f32),
        ],
        scratch_shapes=scratch_like(arrays),
        cost_estimate=cost(2000000000, 4 << 20),
        compiler_params=pltpu.CompilerParams(vmem_limit_bytes=VMEM_LIMIT),
        name="row_side",
    )(x, *packs, rate, *in_hbm(arrays))


def readout_kernel(high_ref, low_ref, pv_ref, gate_ref, *rest):
    packs, states, out_ref = rest[:8], rest[8:16], rest[16]
    core = lax.rem(lax.axis_index("tp"), 2)
    own = iota((32, 16, 128), 0) == iota((32, 16, 128), 2) % 32
    pieces = []
    for state in states:
        block = state[pl.ds(pl.multiple_of(512 * core, 512), 512), :]
        read = dot(block, high_ref[...], 1, 0) + dot(block, low_ref[...], 1, 0)
        pieces.append(jnp.sum(jnp.where(own, read.reshape(32, 16, 128), 0.0), axis=0))
    o = jnp.concatenate(pieces, axis=0) + pv_ref[...]
    o = o * lax.rsqrt(jnp.mean(o * o, axis=0, keepdims=True) + epsilon)
    o = (o * gate_ref[...]).astype(bf16)
    out_ref[...] = dot(o, weight_rows(packs, 32), 0, 0).astype(bf16)


def readout(high, low, pv, gate, packs, states):
    return pl.pallas_call(
        readout_kernel,
        in_specs=vmem_specs(20),
        out_specs=pl.BlockSpec(memory_space=pltpu.VMEM),
        out_shape=pltpu.VMEM((128, 2048), bf16),
        cost_estimate=cost(500000000, 3 << 20),
        compiler_params=pltpu.CompilerParams(vmem_limit_bytes=VMEM_LIMIT),
        name="readout",
    )(high, low, pv, gate, *packs, *states)


def total_kernel(part_ref, out_ref):
    total = jnp.sum(part_ref[...].astype(f32), axis=0)
    total = total * lax.rsqrt(jnp.mean(total * total, axis=1, keepdims=True) + epsilon)
    stacked = jnp.concatenate([total[:, 128 * c : 128 * c + 128] for c in range(16)], axis=0)
    out_ref[...] = stacked.T


def sum_heads(parts):
    return pl.pallas_call(
        total_kernel,
        in_specs=vmem_specs(1),
        out_specs=pl.BlockSpec(memory_space=pltpu.VMEM),
        out_shape=pltpu.VMEM((128, 128), f32),
        cost_estimate=cost(1000000, 1 << 19),
        compiler_params=pltpu.CompilerParams(vmem_limit_bytes=VMEM_LIMIT),
        name="sum_heads",
    )(parts)


def final_kernel(x_ref, gain_ref, out_ref, scratch):
    place = iota((128, 16), 0) // 8 == iota((128, 16), 1)
    gain = jnp.sum(jnp.where(place, gain_ref[...].astype(f32), 0.0), axis=1, keepdims=True)
    scratch[...] = x_ref[...].T * gain
    lane = iota((1, 128), 1)
    rows = [scratch[pl.ds(r, 16, 8), :] for r in range(8)]
    blocks = []
    for i in range(4):
        halves = []
        for h in range(2):
            packed = None
            for q in range(4):
                shift = (32 * q - 32 * i) % 128
                moved = roll(rows[4 * h + q], shift) if shift else rows[4 * h + q]
                packed = moved if packed is None else jnp.where(lane // 32 == q, moved, packed)
            halves.append(packed)
        blocks.append(jnp.concatenate(halves, axis=1))
    full = jnp.concatenate(blocks, axis=0).astype(bf16)
    source = iota((256, 256), 0)
    target = iota((256, 256), 1)
    wanted = (source % 8) * 32 + ((source // 8) % 4) * 8 + source // 32
    order = jnp.where(wanted == target, 1.0, 0.0).astype(bf16)
    out_ref[...] = dot(full, order, 1, 0).astype(bf16).reshape(4, 16, 256)


def final_rows(x, gain):
    return pl.pallas_call(
        final_kernel,
        in_specs=vmem_specs(2),
        out_specs=pl.BlockSpec(memory_space=pltpu.VMEM),
        out_shape=jax.ShapeDtypeStruct((4, 16, 256), bf16),
        scratch_shapes=[pltpu.VMEM((128, 128), f32)],
        cost_estimate=cost(10000000, 1 << 18),
        compiler_params=pltpu.CompilerParams(vmem_limit_bytes=VMEM_LIMIT),
        name="final_rows",
    )(x, gain)


def chip_permute(x, d):
    return lax.ppermute(x, "tp", [((i + 2 * d) % 8, i) for i in range(8)])


def core_permute(x):
    return lax.ppermute(x, "tp", [(i ^ 1, i) for i in range(8)])


def whole_step(
    tokens,
    input_norm_gain,
    query_weight,
    key_weight,
    value_weight,
    output_gate_weight,
    strength_weight,
    decay_weight,
    head_decay_rate,
    proposal_log_decay,
    head_norm_gain,
    output_weight,
    output_norm_gain,
    state,
    previous_keys,
    previous_values,
    previous_log_decay,
    previous_strengths,
    accepted,
    parent,
):
    sent, pack = prepare(
        jnp.transpose(tokens, (1, 2, 0)),
        jnp.transpose(value_weight[:, 0, :], (1, 0)),
        jnp.transpose(output_gate_weight[:, 0, :], (1, 0)),
        output_weight[0],
        head_norm_gain.reshape(1, 16),
    )
    near = [pack] + [chip_permute(pack, d) for d in (1, 2, 3)]
    x = lax.all_to_all(sent.reshape(128, 16, 128), BOTH, 0, 0, tiled=True).reshape(2048, 128)
    accepted_state, *lows = new_state(
        state.reshape(256, 16, 128),
        previous_keys.reshape(1024, 128),
        jnp.transpose(previous_values[:, :, 0, :], (1, 2, 0)),
        jnp.transpose(previous_strengths, (1, 2, 0)),
        jnp.transpose(previous_log_decay, (1, 2, 0)),
        accepted.reshape(1, 256),
    )
    near_states = [lows[0]] + [chip_permute(lows[4 - d], d) for d in (1, 2, 3)]
    packs = near + [core_permute(x) for x in near]
    states = near_states + [core_permute(x) for x in near_states]
    rows = row_side(
        x,
        packs,
        head_decay_rate.reshape(1, 1),
        input_norm_gain.reshape(16, 128),
        query_weight,
        key_weight,
        jnp.transpose(strength_weight, (1, 0)),
        jnp.transpose(decay_weight, (1, 0)),
        jnp.transpose(proposal_log_decay, (1, 2, 0)),
        jnp.transpose(parent, (1, 0)),
    )
    part = readout(*rows, packs, states)
    parts = lax.all_to_all(part.reshape(16, 8, 2048), "kv", 0, 0, tiled=True)
    blocks = lax.all_to_all(sum_heads(parts), BOTH, 0, 0, tiled=True)
    out = final_rows(blocks, output_norm_gain.reshape(1, 16))
    return jnp.transpose(out, (2, 0, 1)), accepted_state.reshape(state.shape)


def solution(mesh):
    placed = (
        P(None, None, ("kv", "tp")),
        P(),
        P(None, "kv"),
        P(None, "kv"),
        P(None, "kv", "tp"),
        P(None, "kv", "tp"),
        P(None, "kv"),
        P(None, "kv"),
        P("kv"),
        P(None, None, "kv"),
        P("tp"),
        P("kv", "tp", None),
        P(("kv", "tp")),
        P(None, "kv", "tp", None),
        P(None, None, "kv"),
        P(None, None, "kv", "tp"),
        P(None, None, "kv"),
        P(None, None, "kv"),
        P(),
        P(),
    )
    return jax.shard_map(
        whole_step,
        mesh=mesh,
        in_specs=placed,
        out_specs=(P(None, None, ("kv", "tp")), P(None, "kv", "tp", None)),
        check_vma=False,
    )
```

```python
import jax
import jax.numpy as jnp
from jax import lax
from jax.experimental import pallas as pl
from jax.experimental.pallas import tpu as pltpu
from jax.sharding import PartitionSpec as P


epsilon = 1e-06
f32 = jnp.float32
bf16 = jnp.bfloat16
BOTH = ("kv", "tp")
VMEM_LIMIT = 16 << 20
PACK = 784


def dot(a, b, ca, cb):
    return lax.dot_general(a, b, (((ca,), (cb,)), ((), ())), preferred_element_type=f32)


def iota(shape, dim):
    return lax.broadcasted_iota(jnp.int32, shape, dim)


def roll(x, shift):
    return pltpu.roll(x, shift, 1)


def split(x):
    hi = x.astype(bf16)
    return hi, (x - hi.astype(f32)).astype(bf16)


def cost(flops, size):
    return pl.CostEstimate(flops=flops, bytes_accessed=size, transcendentals=0)


def chunk_lanes(rows, group):
    lane = iota((1, 128), 1)
    packed = None
    for j in range(4):
        if isinstance(group, int):
            half = rows[j][:, 128 * (group // 4) : 128 * (group // 4) + 128]
            shift = (32 * j - 32 * (group % 4)) % 128
            moved = roll(half, shift) if shift else half
        else:
            half = jnp.where(group >= 4, rows[j][:, 128:], rows[j][:, :128])
            moved = roll(half, lax.rem(32 * j + 128 - 32 * lax.rem(group, 4), 128))
        packed = moved if packed is None else jnp.where(lane // 32 == j, moved, packed)
    return packed


def solve(rhs, coupling):
    x = rhs
    for _ in range(3):
        x = rhs - sum(coupling[d] * roll(x, 32 * d) for d in (1, 2, 3))
    return x


def hbm_specs(count):
    return [pl.BlockSpec(memory_space=pltpu.HBM)] * count


def vmem_specs(count):
    return [pl.BlockSpec(memory_space=pltpu.VMEM)] * count


def start_all(copies):
    for copy in copies:
        copy.start()


def wait_all(copies):
    for copy in copies:
        copy.wait()


def copies_in(sources, targets, sems):
    return [pltpu.make_async_copy(x, y, sems.at[i]) for i, (x, y) in enumerate(zip(sources, targets))]


def in_hbm(arrays):
    return [pltpu.with_memory_space_constraint(x, pltpu.HBM) for x in arrays]


def scratch_like(arrays):
    return [pltpu.VMEM(x.shape, x.dtype) for x in arrays] + [pltpu.SemaphoreType.DMA((len(arrays),))]


def prepare_kernel(*refs):
    sources, state_source, (sent_ref, pack_ref), kept, rest = refs[:15], refs[15], refs[16:18], refs[18:28], refs[28:]
    low_ref, held, sems, state_ref = rest[0], rest[1:6], rest[6:9], rest[9]
    copies = copies_in(sources[:5], held, sems[0])
    ahead = copies_in(sources[5:], kept, sems[1])
    chip = lax.axis_index("tp") // 2
    for i in range(3):
        rows = pl.ds(pl.multiple_of(64 * lax.rem(chip + 1 + i, 4), 64), 64)
        ahead.append(pltpu.make_async_copy(state_source.at[rows], state_ref.at[pl.ds(64 * i, 64)], sems[2].at[i]))
    start_all(copies + ahead)
    wait_all(copies[1:])
    pack_weights(*held[1:], pack_ref)
    copies[0].wait()
    rows = [held[0][i].astype(f32) for i in range(4)]
    for t in range(8):
        block = chunk_lanes(rows, t).astype(bf16)
        for k in range(16):
            sent_ref[k, t] = block
    wait_all(ahead)
    for i in range(6):
        low_ref[512 * i : 512 * i + 512, :] = state_ref[32 * i : 32 * i + 32].reshape(512, 128).astype(bf16)


def prepare(first, ahead, state):
    return pl.pallas_call(
        prepare_kernel,
        in_specs=hbm_specs(16),
        out_specs=vmem_specs(13),
        out_shape=[pltpu.VMEM((16, 8, 16, 128), bf16), pltpu.VMEM((PACK, 128), bf16)]
        + [pltpu.VMEM(x.shape, x.dtype) for x in ahead]
        + [pltpu.VMEM((3072, 128), bf16)],
        scratch_shapes=scratch_like(first)
        + [pltpu.SemaphoreType.DMA((10,)), pltpu.SemaphoreType.DMA((3,)), pltpu.VMEM((192, 16, 128), f32)],
        cost_estimate=cost(10000000, 1 << 20),
        compiler_params=pltpu.CompilerParams(vmem_limit_bytes=VMEM_LIMIT),
        name="prepare",
    )(*in_hbm((*first, *ahead, state)))


def stack(rows):
    return jnp.concatenate(rows, axis=0)


def spread_rows(x):
    count = x.shape[0]
    return jnp.broadcast_to(x[:, None, :], (count, 16, 128)).reshape(16 * count, 128)


def state_update(chips, operands, read, emit):
    key_ref, value_ref, strength_ref, decay_ref, accepted_ref = operands
    steps = range(2 * len(chips))
    chip = lax.axis_index("tp") // 2
    groups = [2 * lax.rem(chip + chips[step // 2], 4) + step % 2 for step in steps]
    lane = iota((1, 128), 1)
    place = lane // 32
    strength = stack([chunk_lanes([strength_ref[j] for j in range(4)], x) for x in groups])
    decay = stack([chunk_lanes([decay_ref[j] for j in range(4)], x) for x in groups])
    accepted = stack([chunk_lanes([accepted_ref[...].astype(f32)] * 4, x) for x in groups])
    values = [value_ref[j].astype(f32) for j in range(4)]
    values = stack([chunk_lanes(values, x) for x in groups])
    live = jnp.where(place < accepted, 1.0, 0.0)
    beta = strength * live
    g = decay * live
    gam = g + sum(jnp.where(place >= d, roll(g, 32 * d), 0.0) for d in (1, 2, 3))
    last = g + sum(roll(g, 32 * d) for d in (1, 2, 3))
    row = iota((128, 128), 0)
    column = iota((128, 128), 1)
    order = jnp.where(column == (row % 32) * 4 + row // 32, 1.0, 0.0).astype(bf16)
    keys = [dot(order, key_ref[pl.ds(pl.multiple_of(128 * x, 128), 128), :], 1, 0).astype(bf16) for x in groups]
    grams = [dot(x, x, 1, 1) for x in keys]

    def diagonal(d):
        return stack(
            [jnp.sum(jnp.where(row == column - 32 * d, gram, 0.0), axis=0, keepdims=True) for gram in grams]
        )

    unit = lax.rsqrt(diagonal(0) + epsilon)
    coupling = {
        d: jnp.where(
            place >= d,
            beta * diagonal(d) * unit * roll(unit, 32 * d) * jnp.exp(jnp.minimum(gam - roll(gam, 32 * d), 0.0)),
            0.0,
        )
        for d in (1, 2, 3)
    }
    coupling = {d: spread_rows(x) for d, x in coupling.items()}
    own = iota((32, 16, 128), 0) == iota((32, 16, 128), 2) % 32
    seen = []
    for step in steps:
        product = dot(read(step).astype(bf16), keys[step], 1, 1)
        seen.append(jnp.sum(jnp.where(own, product.reshape(32, 16, 128), 0.0), axis=0))
    update = solve(spread_rows(beta) * values - spread_rows(beta * jnp.exp(gam) * unit) * stack(seen), coupling)
    update = update * spread_rows(jnp.exp(last - gam) * unit)
    keep = jnp.exp(last)
    for step in steps:
        spread = jnp.broadcast_to(update[16 * step : 16 * step + 16][None], (32, 16, 128))
        change = dot(jnp.where(own, spread, 0.0).reshape(512, 128).astype(bf16), keys[step], 1, 0)
        kept = jnp.where(iota((32, 128), 0) == iota((32, 128), 1), keep[step : step + 1], 0.0)
        kept = jnp.broadcast_to(jnp.sum(kept, axis=1, keepdims=True), (32, 128))
        kept = jnp.broadcast_to(kept[:, None, :], (32, 16, 128))
        emit(step, kept.reshape(512, 128) * read(step).astype(f32) + change)


def other_chips_kernel(state_ref, *refs):
    operands, lows = refs[:5], refs[5:]

    def emit(step, new):
        lows[step // 2][512 * (step % 2) : 512 * (step % 2) + 512, :] = new.astype(bf16)

    state_update((1, 2, 3), operands, lambda step: state_ref[512 * step : 512 * step + 512, :], emit)


def other_chips_state(state, operands):
    return pl.pallas_call(
        other_chips_kernel,
        in_specs=vmem_specs(6),
        out_specs=vmem_specs(3),
        out_shape=[pltpu.VMEM((1024, 128), bf16)] * 3,
        cost_estimate=cost(1500000000, 3 << 20),
        compiler_params=pltpu.CompilerParams(vmem_limit_bytes=VMEM_LIMIT),
        name="other_chips_state",
    )(state, *operands)


def all_chips_kernel(source, key_source, *refs):
    operands, (state_out, low_ref, state_ref, key_ref, sems) = refs[:4], refs[4:]
    chip = lax.axis_index("tp") // 2

    def rows_of(i):
        return pl.ds(pl.multiple_of(64 * lax.rem(chip + i, 4), 64), 64)

    def held(i):
        return pl.ds(64 * i, 64)

    loads = [pltpu.make_async_copy(source.at[rows_of(i)], state_ref.at[held(i)], sems.at[0, i]) for i in range(4)]
    stores = [pltpu.make_async_copy(state_ref.at[held(i)], state_out.at[rows_of(i)], sems.at[1, i]) for i in range(4)]
    keys = pltpu.make_async_copy(key_source, key_ref, sems.at[0, 4])
    keys.start()
    start_all(loads)
    keys.wait()
    arrived = set()

    def read(step):
        if step // 2 not in arrived:
            arrived.add(step // 2)
            loads[step // 2].wait()
        return state_ref[32 * step : 32 * step + 32].reshape(512, 128)

    def emit(step, new):
        state_ref[32 * step : 32 * step + 32] = new.reshape(32, 16, 128)
        if step < 2:
            low_ref[512 * step : 512 * step + 512, :] = new.astype(bf16)
        if step % 2 == 1:
            stores[step // 2].start()

    state_update((0, 1, 2, 3), (key_ref, *operands), read, emit)
    wait_all(stores)


def all_chips_state(state, keys, operands):
    return pl.pallas_call(
        all_chips_kernel,
        in_specs=hbm_specs(2) + vmem_specs(4),
        out_specs=hbm_specs(1) + vmem_specs(1),
        out_shape=[pltpu.HBM((256, 16, 128), f32), pltpu.VMEM((1024, 128), bf16)],
        scratch_shapes=[
            pltpu.VMEM((256, 16, 128), f32),
            pltpu.VMEM((1024, 128), bf16),
            pltpu.SemaphoreType.DMA((2, 5)),
        ],
        cost_estimate=cost(2000000000, 4 << 20),
        compiler_params=pltpu.CompilerParams(vmem_limit_bytes=VMEM_LIMIT),
        name="all_chips_state",
    )(*in_hbm((state, keys)), *operands)


def pack_weights(value_ref, gate_ref, output_ref, gain_ref, pack_ref):
    row = iota((16, 16), 0)
    gain = jnp.where(row == iota((16, 16), 1), jnp.broadcast_to(gain_ref[...].astype(f32), (16, 16)), 0.0)
    gain = jnp.broadcast_to(jnp.sum(gain, axis=1, keepdims=True), (16, 128)).astype(bf16)
    source = iota((128, 128), 0)
    target = iota((128, 128), 1)
    order = jnp.where(target == (source % 16) * 8 + source // 16, 1.0, 0.0).astype(bf16)
    rows = jnp.concatenate([output_ref[:, 128 * b : 128 * b + 128] for b in range(16)], axis=0)
    rows = dot(rows, order, 1, 0)
    lane = iota((1, 128), 1)
    for c in range(16):
        packed = None
        for b in range(16):
            piece = rows[16 * b : 16 * b + 16, :]
            shift = (8 * (b - c)) % 128
            moved = roll(piece, shift) if shift else piece
            packed = moved if packed is None else jnp.where(lane // 8 == b, moved, packed)
        columns = slice(128 * c, 128 * c + 128)
        block = jnp.concatenate([value_ref[:, columns], gate_ref[:, columns], packed.astype(bf16)], axis=0)
        pack_ref[48 * c : 48 * c + 48, :] = block
    pack_ref[768:, :] = gain


def weight_rows(packs, first):
    return jnp.concatenate(
        [
            jnp.concatenate([x[48 * b + first : 48 * b + first + 16, :] for x in packs], axis=0)
            for b in range(16)
        ],
        axis=1,
    )


def rows_kernel(x_ref, *refs):
    packs, small, rate_ref, sources, outs, held, sems = (
        refs[:8], refs[8:13], refs[13], refs[14:16], refs[16:20], refs[20:22], refs[22],
    )
    gain_ref, strength_ref, decay_ref, log_decay_ref, parent_ref = small
    high_ref, low_ref, pv_ref, gate_ref = outs
    wq_ref, wk_ref = held
    copies = copies_in(sources, held, sems)
    start_all(copies)
    group = lax.axis_index("tp")
    x = x_ref[...].astype(f32)
    scale = lax.rsqrt(jnp.mean(x * x, axis=0, keepdims=True) + epsilon)
    column = iota((128, 128), 1) == iota((128, 128), 0)
    gain = jnp.concatenate(
        [jnp.where(column, gain_ref[b : b + 1, :].astype(f32), 0.0).astype(bf16) for b in range(16)], axis=0
    )
    gain = dot(gain, jnp.ones((128, 128), bf16), 1, 0)
    normed = (x * scale * gain).astype(bf16)

    def project(weight, dim):
        return dot(weight, normed, dim, 0)

    def rounded(x):
        return x.astype(bf16).astype(f32)

    first = iota((16, 2048), 0) == 0
    scalars = jnp.where(first, strength_ref[...].astype(f32), decay_ref[...].astype(f32))
    scalars = scalars.astype(bf16)
    both = jnp.concatenate([weight_rows(packs, 0), weight_rows(packs, 16)], axis=0)
    both = rounded(project(both, 1))
    values, zgate = both[:128], both[128:]
    logits = project(scalars, 1)
    wait_all(copies)
    queries = rounded(project(wq_ref[...], 0))
    keys = rounded(project(wk_ref[...], 0))
    gain = jnp.concatenate([pack[768:, :] for pack in packs], axis=0).astype(f32)

    def unit(x):
        return x * lax.rsqrt(jnp.sum(x * x, axis=0, keepdims=True) + epsilon)

    queries = unit(queries) * 128**-0.5
    keys = unit(keys)
    beta = jax.nn.sigmoid(logits[0:1, :])
    pre = logits[1:2, :]
    softplus = jnp.maximum(pre, 0.0) + jnp.log1p(jnp.exp(-jnp.abs(pre)))
    log_decay = chunk_lanes([log_decay_ref[i] for i in range(4)], group)
    parent = chunk_lanes([parent_ref[i : i + 1, :].astype(f32) for i in range(4)], group)
    g = log_decay - rate_ref[0, 0] * softplus
    place = (iota((1, 128), 1) // 32).astype(f32)
    hit = {d: jnp.where((parent == place - d) & (place >= d), 1.0, 0.0) for d in (1, 2, 3)}
    seen = {1: hit[1]}
    seen[2] = hit[2] + hit[1] * roll(seen[1], 32)
    seen[3] = hit[3] + hit[1] * roll(seen[2], 32) + hit[2] * roll(seen[1], 64)
    gam = g + sum(seen[d] * roll(g, 32 * d) for d in (1, 2, 3))
    coupling, reach = {}, {0: jnp.sum(queries * keys, axis=0, keepdims=True)}
    for d in (1, 2, 3):
        earlier = roll(keys, 32 * d)
        weight = jnp.exp(jnp.minimum(gam - roll(gam, 32 * d), 0.0)) * seen[d]
        coupling[d] = beta * weight * jnp.sum(keys * earlier, axis=0, keepdims=True)
        reach[d] = weight * jnp.sum(queries * earlier, axis=0, keepdims=True)
    solved_values = solve(beta * values, coupling)
    solved_keys = solve((beta * jnp.exp(gam)) * keys, coupling)

    def reached(x):
        return reach[0] * x + sum(reach[d] * roll(x, 32 * d) for d in (1, 2, 3))

    probe = jnp.exp(gam) * queries - reached(solved_keys)
    high_ref[...], low_ref[...] = split(probe)
    pv_ref[...] = reached(solved_values)
    gate_ref[...] = gain * (zgate * jax.nn.sigmoid(zgate))


def row_side(x, packs, small, rate, *weights):
    return pl.pallas_call(
        rows_kernel,
        in_specs=vmem_specs(14) + [pl.BlockSpec(memory_space=pltpu.SMEM)] + hbm_specs(2),
        out_specs=vmem_specs(4),
        out_shape=[
            pltpu.VMEM((128, 128), bf16),
            pltpu.VMEM((128, 128), bf16),
            pltpu.VMEM((128, 128), f32),
            pltpu.VMEM((128, 128), f32),
        ],
        scratch_shapes=scratch_like(weights),
        cost_estimate=cost(2000000000, 4 << 20),
        compiler_params=pltpu.CompilerParams(vmem_limit_bytes=VMEM_LIMIT),
        name="row_side",
    )(x, *packs, *small, rate, *in_hbm(weights))


def readout_kernel(high_ref, low_ref, pv_ref, gate_ref, *rest):
    packs, states, out_ref = rest[:8], rest[8:16], rest[16]
    core = lax.rem(lax.axis_index("tp"), 2)
    own = iota((32, 16, 128), 0) == iota((32, 16, 128), 2) % 32
    pieces = []
    for state in states:
        block = state[pl.ds(pl.multiple_of(512 * core, 512), 512), :]
        read = dot(block, high_ref[...], 1, 0) + dot(block, low_ref[...], 1, 0)
        pieces.append(jnp.sum(jnp.where(own, read.reshape(32, 16, 128), 0.0), axis=0))
    o = jnp.concatenate(pieces, axis=0) + pv_ref[...]
    o = o * lax.rsqrt(jnp.mean(o * o, axis=0, keepdims=True) + epsilon)
    o = (o * gate_ref[...]).astype(bf16)
    out_ref[...] = dot(o, weight_rows(packs, 32), 0, 0).astype(bf16)


def readout(high, low, pv, gate, packs, states):
    return pl.pallas_call(
        readout_kernel,
        in_specs=vmem_specs(20),
        out_specs=pl.BlockSpec(memory_space=pltpu.VMEM),
        out_shape=pltpu.VMEM((128, 2048), bf16),
        cost_estimate=cost(500000000, 3 << 20),
        compiler_params=pltpu.CompilerParams(vmem_limit_bytes=VMEM_LIMIT),
        name="readout",
    )(high, low, pv, gate, *packs, *states)


def total_kernel(part_ref, out_ref):
    total = jnp.sum(part_ref[...].astype(f32), axis=0)
    total = total * lax.rsqrt(jnp.mean(total * total, axis=1, keepdims=True) + epsilon)
    stacked = jnp.concatenate([total[:, 128 * c : 128 * c + 128] for c in range(16)], axis=0)
    out_ref[...] = stacked.T


def sum_heads(parts):
    return pl.pallas_call(
        total_kernel,
        in_specs=vmem_specs(1),
        out_specs=pl.BlockSpec(memory_space=pltpu.VMEM),
        out_shape=pltpu.VMEM((128, 128), f32),
        cost_estimate=cost(1000000, 1 << 19),
        compiler_params=pltpu.CompilerParams(vmem_limit_bytes=VMEM_LIMIT),
        name="sum_heads",
    )(parts)


def final_kernel(x_ref, gain_ref, out_ref, scratch):
    place = iota((128, 16), 0) // 8 == iota((128, 16), 1)
    gain = jnp.sum(jnp.where(place, gain_ref[...].astype(f32), 0.0), axis=1, keepdims=True)
    scratch[...] = x_ref[...].T * gain
    lane = iota((1, 128), 1)
    rows = [scratch[pl.ds(r, 16, 8), :] for r in range(8)]
    blocks = []
    for i in range(4):
        halves = []
        for h in range(2):
            packed = None
            for q in range(4):
                shift = (32 * q - 32 * i) % 128
                moved = roll(rows[4 * h + q], shift) if shift else rows[4 * h + q]
                packed = moved if packed is None else jnp.where(lane // 32 == q, moved, packed)
            halves.append(packed)
        blocks.append(jnp.concatenate(halves, axis=1))
    full = jnp.concatenate(blocks, axis=0).astype(bf16)
    source = iota((256, 256), 0)
    target = iota((256, 256), 1)
    wanted = (source % 8) * 32 + ((source // 8) % 4) * 8 + source // 32
    order = jnp.where(wanted == target, 1.0, 0.0).astype(bf16)
    out_ref[...] = dot(full, order, 1, 0).astype(bf16).reshape(4, 16, 256)


def final_rows(x, gain):
    return pl.pallas_call(
        final_kernel,
        in_specs=vmem_specs(2),
        out_specs=pl.BlockSpec(memory_space=pltpu.VMEM),
        out_shape=jax.ShapeDtypeStruct((4, 16, 256), bf16),
        scratch_shapes=[pltpu.VMEM((128, 128), f32)],
        cost_estimate=cost(10000000, 1 << 18),
        compiler_params=pltpu.CompilerParams(vmem_limit_bytes=VMEM_LIMIT),
        name="final_rows",
    )(x, gain)


def chip_permute(x, d):
    return lax.ppermute(x, "tp", [((i + 2 * d) % 8, i) for i in range(8)])


def core_permute(x):
    return lax.ppermute(x, "tp", [(i ^ 1, i) for i in range(8)])


def whole_step(
    tokens,
    input_norm_gain,
    query_weight,
    key_weight,
    value_weight,
    output_gate_weight,
    strength_weight,
    decay_weight,
    head_decay_rate,
    proposal_log_decay,
    head_norm_gain,
    output_weight,
    output_norm_gain,
    state,
    previous_keys,
    previous_values,
    previous_log_decay,
    previous_strengths,
    accepted,
    parent,
):
    sent, pack, *ahead, other_rows = prepare(
        (
            jnp.transpose(tokens, (1, 2, 0)),
            jnp.transpose(value_weight[:, 0, :], (1, 0)),
            jnp.transpose(output_gate_weight[:, 0, :], (1, 0)),
            output_weight[0],
            head_norm_gain.reshape(1, 16),
        ),
        (
            previous_keys.reshape(1024, 128),
            jnp.transpose(previous_values[:, :, 0, :], (1, 2, 0)),
            jnp.transpose(previous_strengths, (1, 2, 0)),
            jnp.transpose(previous_log_decay, (1, 2, 0)),
            accepted.reshape(1, 256),
            input_norm_gain.reshape(16, 128),
            jnp.transpose(strength_weight, (1, 0)),
            jnp.transpose(decay_weight, (1, 0)),
            jnp.transpose(proposal_log_decay, (1, 2, 0)),
            jnp.transpose(parent, (1, 0)),
        ),
        state.reshape(256, 16, 128),
    )
    ahead, small = ahead[:5], ahead[5:]
    near = [pack] + [chip_permute(pack, d) for d in (1, 2, 3)]
    x = lax.all_to_all(sent.reshape(128, 16, 128), BOTH, 0, 0, tiled=True).reshape(2048, 128)
    lows = other_chips_state(other_rows, ahead)
    accepted_state, own_low = all_chips_state(state.reshape(256, 16, 128), previous_keys.reshape(1024, 128), ahead[1:])
    near_states = [own_low] + [chip_permute(lows[3 - d], d) for d in (1, 2, 3)]
    packs = near + [core_permute(x) for x in near]
    states = near_states + [core_permute(x) for x in near_states]
    rows = row_side(x, packs, small, head_decay_rate.reshape(1, 1), query_weight, key_weight)
    part = readout(*rows, packs, states)
    parts = lax.all_to_all(part.reshape(16, 8, 2048), "kv", 0, 0, tiled=True)
    blocks = lax.all_to_all(sum_heads(parts), BOTH, 0, 0, tiled=True)
    out = final_rows(blocks, output_norm_gain.reshape(1, 16))
    return jnp.transpose(out, (2, 0, 1)), accepted_state.reshape(state.shape)


def solution(mesh):
    placed = (
        P(None, None, ("kv", "tp")),
        P(),
        P(None, "kv"),
        P(None, "kv"),
        P(None, "kv", "tp"),
        P(None, "kv", "tp"),
        P(None, "kv"),
        P(None, "kv"),
        P("kv"),
        P(None, None, "kv"),
        P("tp"),
        P("kv", "tp", None),
        P(("kv", "tp")),
        P(None, "kv", "tp", None),
        P(None, None, "kv"),
        P(None, None, "kv", "tp"),
        P(None, None, "kv"),
        P(None, None, "kv"),
        P(),
        P(),
    )
    return jax.shard_map(
        whole_step,
        mesh=mesh,
        in_specs=placed,
        out_specs=(P(None, None, ("kv", "tp")), P(None, "kv", "tp", None)),
        check_vma=False,
    )
```

```python
import jax
import jax.numpy as jnp
from jax import lax
from jax.experimental import pallas as pl
from jax.experimental.pallas import tpu as pltpu
from jax.sharding import PartitionSpec as P


epsilon = 1e-06
f32 = jnp.float32
bf16 = jnp.bfloat16
BOTH = ("kv", "tp")
VMEM_LIMIT = 16 << 20
PACK = 784
BUNDLE = 1024 + PACK


def dot(a, b, ca, cb):
    return lax.dot_general(a, b, (((ca,), (cb,)), ((), ())), preferred_element_type=f32)


def iota(shape, dim):
    return lax.broadcasted_iota(jnp.int32, shape, dim)


def roll(x, shift):
    return pltpu.roll(x, shift, 1)


def cost(flops, size):
    return pl.CostEstimate(flops=flops, bytes_accessed=size, transcendentals=0)


def chunk_lanes(rows, group):
    lane = iota((1, 128), 1)
    packed = None
    for j in range(4):
        if isinstance(group, int):
            half = rows[j][:, 128 * (group // 4) : 128 * (group // 4) + 128]
            shift = (32 * j - 32 * (group % 4)) % 128
            moved = roll(half, shift) if shift else half
        else:
            half = jnp.where(group >= 4, rows[j][:, 128:], rows[j][:, :128])
            moved = roll(half, lax.rem(32 * j + 128 - 32 * lax.rem(group, 4), 128))
        packed = moved if packed is None else jnp.where(lane // 32 == j, moved, packed)
    return packed


def solve(rhs, coupling):
    x = rhs
    for _ in range(3):
        x = rhs - sum(coupling[d] * roll(x, 32 * d) for d in (1, 2, 3))
    return x


def hbm_specs(count):
    return [pl.BlockSpec(memory_space=pltpu.HBM)] * count


def vmem_specs(count):
    return [pl.BlockSpec(memory_space=pltpu.VMEM)] * count


def start_all(copies):
    for copy in copies:
        copy.start()


def wait_all(copies):
    for copy in copies:
        copy.wait()


def copies_in(sources, targets, sems):
    return [pltpu.make_async_copy(x, y, sems.at[i]) for i, (x, y) in enumerate(zip(sources, targets))]


def in_hbm(arrays):
    return [pltpu.with_memory_space_constraint(x, pltpu.HBM) for x in arrays]


def scratch_like(arrays):
    return [pltpu.VMEM(x.shape, x.dtype) for x in arrays] + [pltpu.SemaphoreType.DMA((len(arrays),))]


def prepare_kernel(*refs):
    sources, state_source, (sent_ref, pack_ref, bundle_ref), kept, rest = (
        refs[:15], refs[15], refs[16:19], refs[19:29], refs[29:],
    )
    low_ref, held, sems, state_ref = rest[0], rest[1:6], rest[6:9], rest[9]
    copies = copies_in(sources[:5], held, sems[0])
    ahead = copies_in(sources[5:], kept, sems[1])
    chip = lax.axis_index("tp") // 2
    loads = []
    for i, offset in enumerate((2, 1, 3)):
        rows = pl.ds(pl.multiple_of(64 * lax.rem(chip + offset, 4), 64), 64)
        loads.append(pltpu.make_async_copy(state_source.at[rows], state_ref.at[pl.ds(64 * i, 64)], sems[2].at[i]))
    start_all(copies + ahead + loads)
    wait_all(copies[1:])
    pack_weights(*held[1:], pack_ref)
    bundle_ref[1024:, :] = pack_ref[...]
    copies[0].wait()
    rows = [held[0][i].astype(f32) for i in range(4)]
    for t in range(8):
        block = chunk_lanes(rows, t).astype(bf16)
        for k in range(16):
            sent_ref[k, t] = block
    wait_all(ahead + loads[:1])

    def read(step):
        return state_ref[32 * step : 32 * step + 32].reshape(512, 128)

    def emit(step, new):
        bundle_ref[512 * step : 512 * step + 512, :] = new.astype(bf16)

    state_update((2,), kept[:5], read, emit)
    wait_all(loads[1:])
    for i in range(4):
        low_ref[512 * i : 512 * i + 512, :] = read(2 + i).astype(bf16)


def prepare(first, ahead, state):
    return pl.pallas_call(
        prepare_kernel,
        in_specs=hbm_specs(16),
        out_specs=vmem_specs(14),
        out_shape=[pltpu.VMEM((16, 8, 16, 128), bf16), pltpu.VMEM((PACK, 128), bf16), pltpu.VMEM((BUNDLE, 128), bf16)]
        + [pltpu.VMEM(x.shape, x.dtype) for x in ahead]
        + [pltpu.VMEM((2048, 128), bf16)],
        scratch_shapes=scratch_like(first)
        + [pltpu.SemaphoreType.DMA((10,)), pltpu.SemaphoreType.DMA((3,)), pltpu.VMEM((192, 16, 128), f32)],
        cost_estimate=cost(10000000, 1 << 20),
        compiler_params=pltpu.CompilerParams(vmem_limit_bytes=VMEM_LIMIT),
        name="prepare",
    )(*in_hbm((*first, *ahead, state)))


def stack(rows):
    return jnp.concatenate(rows, axis=0)


def spread_rows(x):
    count = x.shape[0]
    return jnp.broadcast_to(x[:, None, :], (count, 16, 128)).reshape(16 * count, 128)


def state_update(chips, operands, read, emit):
    key_ref, value_ref, strength_ref, decay_ref, accepted_ref = operands
    steps = range(2 * len(chips))
    chip = lax.axis_index("tp") // 2
    groups = [2 * lax.rem(chip + chips[step // 2], 4) + step % 2 for step in steps]
    lane = iota((1, 128), 1)
    place = lane // 32
    strength = stack([chunk_lanes([strength_ref[j] for j in range(4)], x) for x in groups])
    decay = stack([chunk_lanes([decay_ref[j] for j in range(4)], x) for x in groups])
    accepted = stack([chunk_lanes([accepted_ref[...].astype(f32)] * 4, x) for x in groups])
    values = [value_ref[j].astype(f32) for j in range(4)]
    values = stack([chunk_lanes(values, x) for x in groups])
    live = jnp.where(place < accepted, 1.0, 0.0)
    beta = strength * live
    g = decay * live
    gam = g + sum(jnp.where(place >= d, roll(g, 32 * d), 0.0) for d in (1, 2, 3))
    last = g + sum(roll(g, 32 * d) for d in (1, 2, 3))
    row = iota((128, 128), 0)
    column = iota((128, 128), 1)
    order = jnp.where(column == (row % 32) * 4 + row // 32, 1.0, 0.0).astype(bf16)
    keys = [dot(order, key_ref[pl.ds(pl.multiple_of(128 * x, 128), 128), :], 1, 0).astype(bf16) for x in groups]
    grams = [dot(x, x, 1, 1) for x in keys]

    def diagonal(d):
        return stack(
            [jnp.sum(jnp.where(row == column - 32 * d, gram, 0.0), axis=0, keepdims=True) for gram in grams]
        )

    unit = lax.rsqrt(diagonal(0) + epsilon)
    coupling = {
        d: jnp.where(
            place >= d,
            beta * diagonal(d) * unit * roll(unit, 32 * d) * jnp.exp(jnp.minimum(gam - roll(gam, 32 * d), 0.0)),
            0.0,
        )
        for d in (1, 2, 3)
    }
    coupling = {d: spread_rows(x) for d, x in coupling.items()}
    own = iota((32, 16, 128), 0) == iota((32, 16, 128), 2) % 32
    seen = []
    for step in steps:
        product = dot(read(step).astype(bf16), keys[step], 1, 1)
        seen.append(jnp.sum(jnp.where(own, product.reshape(32, 16, 128), 0.0), axis=0))
    update = solve(spread_rows(beta) * values - spread_rows(beta * jnp.exp(gam) * unit) * stack(seen), coupling)
    update = update * spread_rows(jnp.exp(last - gam) * unit)
    keep = jnp.exp(last)
    for step in steps:
        spread = jnp.broadcast_to(update[16 * step : 16 * step + 16][None], (32, 16, 128))
        change = dot(jnp.where(own, spread, 0.0).reshape(512, 128).astype(bf16), keys[step], 1, 0)
        kept = jnp.where(iota((32, 128), 0) == iota((32, 128), 1), keep[step : step + 1], 0.0)
        kept = jnp.broadcast_to(jnp.sum(kept, axis=1, keepdims=True), (32, 128))
        kept = jnp.broadcast_to(kept[:, None, :], (32, 16, 128))
        emit(step, kept.reshape(512, 128) * read(step).astype(f32) + change)


def other_chips_kernel(state_ref, *refs):
    operands, lows = refs[:5], refs[5:]

    def emit(step, new):
        lows[step // 2][512 * (step % 2) : 512 * (step % 2) + 512, :] = new.astype(bf16)

    state_update((1, 3), operands, lambda step: state_ref[512 * step : 512 * step + 512, :], emit)


def other_chips_state(state, operands):
    return pl.pallas_call(
        other_chips_kernel,
        in_specs=vmem_specs(6),
        out_specs=vmem_specs(2),
        out_shape=[pltpu.VMEM((1024, 128), bf16)] * 2,
        cost_estimate=cost(1000000000, 2 << 20),
        compiler_params=pltpu.CompilerParams(vmem_limit_bytes=VMEM_LIMIT),
        name="other_chips_state",
    )(state, *operands)


def all_chips_kernel(source, key_source, *refs):
    operands, (state_out, low_ref, state_ref, key_ref, sems) = refs[:4], refs[4:]
    chip = lax.axis_index("tp") // 2

    def rows_of(i):
        return pl.ds(pl.multiple_of(64 * lax.rem(chip + i, 4), 64), 64)

    def held(i):
        return pl.ds(64 * i, 64)

    loads = [pltpu.make_async_copy(source.at[rows_of(i)], state_ref.at[held(i)], sems.at[0, i]) for i in range(4)]
    stores = [pltpu.make_async_copy(state_ref.at[held(i)], state_out.at[rows_of(i)], sems.at[1, i]) for i in range(4)]
    keys = pltpu.make_async_copy(key_source, key_ref, sems.at[0, 4])
    keys.start()
    start_all(loads)
    keys.wait()
    arrived = set()

    def read(step):
        if step // 2 not in arrived:
            arrived.add(step // 2)
            loads[step // 2].wait()
        return state_ref[32 * step : 32 * step + 32].reshape(512, 128)

    def emit(step, new):
        state_ref[32 * step : 32 * step + 32] = new.reshape(32, 16, 128)
        if step < 2:
            low_ref[512 * step : 512 * step + 512, :] = new.astype(bf16)
        if step % 2 == 1:
            stores[step // 2].start()

    state_update((0, 1, 2, 3), (key_ref, *operands), read, emit)
    wait_all(stores)


def all_chips_state(state, keys, operands):
    return pl.pallas_call(
        all_chips_kernel,
        in_specs=hbm_specs(2) + vmem_specs(4),
        out_specs=hbm_specs(1) + vmem_specs(1),
        out_shape=[pltpu.HBM((256, 16, 128), f32), pltpu.VMEM((1024, 128), bf16)],
        scratch_shapes=[
            pltpu.VMEM((256, 16, 128), f32),
            pltpu.VMEM((1024, 128), bf16),
            pltpu.SemaphoreType.DMA((2, 5)),
        ],
        cost_estimate=cost(2000000000, 4 << 20),
        compiler_params=pltpu.CompilerParams(vmem_limit_bytes=VMEM_LIMIT),
        name="all_chips_state",
    )(*in_hbm((state, keys)), *operands)


def pack_weights(value_ref, gate_ref, output_ref, gain_ref, pack_ref):
    row = iota((16, 16), 0)
    gain = jnp.where(row == iota((16, 16), 1), jnp.broadcast_to(gain_ref[...].astype(f32), (16, 16)), 0.0)
    gain = jnp.broadcast_to(jnp.sum(gain, axis=1, keepdims=True), (16, 128)).astype(bf16)
    source = iota((128, 128), 0)
    target = iota((128, 128), 1)
    order = jnp.where(target == (source % 16) * 8 + source // 16, 1.0, 0.0).astype(bf16)
    rows = jnp.concatenate([output_ref[:, 128 * b : 128 * b + 128] for b in range(16)], axis=0)
    rows = dot(rows, order, 1, 0)
    lane = iota((1, 128), 1)
    for c in range(16):
        packed = None
        for b in range(16):
            piece = rows[16 * b : 16 * b + 16, :]
            shift = (8 * (b - c)) % 128
            moved = roll(piece, shift) if shift else piece
            packed = moved if packed is None else jnp.where(lane // 8 == b, moved, packed)
        columns = slice(128 * c, 128 * c + 128)
        block = jnp.concatenate([value_ref[:, columns], gate_ref[:, columns], packed.astype(bf16)], axis=0)
        pack_ref[48 * c : 48 * c + 48, :] = block
    pack_ref[768:, :] = gain


def pack_rows(ref, first, count):
    base = ref.shape[0] - PACK
    return ref[base + first : base + first + count, :]


def weight_rows(packs, first):
    return jnp.concatenate(
        [stack([pack_rows(x, 48 * b + first, 16) for x in packs]) for b in range(16)],
        axis=1,
    )


def rows_kernel(x_ref, *refs):
    packs, small, rate_ref, sources, outs, held, sems = (
        refs[:8], refs[8:13], refs[13], refs[14:16], refs[16:19], refs[19:21], refs[21],
    )
    gain_ref, strength_ref, decay_ref, log_decay_ref, parent_ref = small
    probe_ref, pv_ref, gate_ref = outs
    wq_ref, wk_ref = held
    copies = copies_in(sources, held, sems)
    start_all(copies)
    group = lax.axis_index("tp")
    x = x_ref[...].astype(f32)
    scale = lax.rsqrt(jnp.mean(x * x, axis=0, keepdims=True) + epsilon)
    column = iota((128, 128), 1) == iota((128, 128), 0)
    gain = jnp.concatenate(
        [jnp.where(column, gain_ref[b : b + 1, :].astype(f32), 0.0).astype(bf16) for b in range(16)], axis=0
    )
    gain = dot(gain, jnp.ones((128, 128), bf16), 1, 0)
    normed = (x * scale * gain).astype(bf16)

    def project(weight, dim):
        return dot(weight, normed, dim, 0)

    def rounded(x):
        return x.astype(bf16).astype(f32)

    first = iota((16, 2048), 0) == 0
    scalars = jnp.where(first, strength_ref[...].astype(f32), decay_ref[...].astype(f32))
    scalars = scalars.astype(bf16)
    both = jnp.concatenate([weight_rows(packs, 0), weight_rows(packs, 16)], axis=0)
    both = rounded(project(both, 1))
    values, zgate = both[:128], both[128:]
    logits = project(scalars, 1)
    wait_all(copies)
    queries = rounded(project(wq_ref[...], 0))
    keys = rounded(project(wk_ref[...], 0))
    gain = jnp.concatenate([pack_rows(pack, 768, 16) for pack in packs], axis=0).astype(f32)

    def unit(x):
        return x * lax.rsqrt(jnp.sum(x * x, axis=0, keepdims=True) + epsilon)

    queries = unit(queries) * 128**-0.5
    keys = unit(keys)
    beta = jax.nn.sigmoid(logits[0:1, :])
    pre = logits[1:2, :]
    softplus = jnp.maximum(pre, 0.0) + jnp.log1p(jnp.exp(-jnp.abs(pre)))
    log_decay = chunk_lanes([log_decay_ref[i] for i in range(4)], group)
    parent = chunk_lanes([parent_ref[i : i + 1, :].astype(f32) for i in range(4)], group)
    g = log_decay - rate_ref[0, 0] * softplus
    place = (iota((1, 128), 1) // 32).astype(f32)
    hit = {d: jnp.where((parent == place - d) & (place >= d), 1.0, 0.0) for d in (1, 2, 3)}
    seen = {1: hit[1]}
    seen[2] = hit[2] + hit[1] * roll(seen[1], 32)
    seen[3] = hit[3] + hit[1] * roll(seen[2], 32) + hit[2] * roll(seen[1], 64)
    gam = g + sum(seen[d] * roll(g, 32 * d) for d in (1, 2, 3))
    coupling, reach = {}, {0: jnp.sum(queries * keys, axis=0, keepdims=True)}
    for d in (1, 2, 3):
        earlier = roll(keys, 32 * d)
        weight = jnp.exp(jnp.minimum(gam - roll(gam, 32 * d), 0.0)) * seen[d]
        coupling[d] = beta * weight * jnp.sum(keys * earlier, axis=0, keepdims=True)
        reach[d] = weight * jnp.sum(queries * earlier, axis=0, keepdims=True)
    solved_values = solve(beta * values, coupling)
    solved_keys = solve((beta * jnp.exp(gam)) * keys, coupling)

    def reached(x):
        return reach[0] * x + sum(reach[d] * roll(x, 32 * d) for d in (1, 2, 3))

    probe = jnp.exp(gam) * queries - reached(solved_keys)
    probe_ref[...] = probe.astype(bf16)
    pv_ref[...] = reached(solved_values)
    gate_ref[...] = gain * (zgate * jax.nn.sigmoid(zgate))


def row_side(x, packs, small, rate, *weights):
    return pl.pallas_call(
        rows_kernel,
        in_specs=vmem_specs(14) + [pl.BlockSpec(memory_space=pltpu.SMEM)] + hbm_specs(2),
        out_specs=vmem_specs(3),
        out_shape=[
            pltpu.VMEM((128, 128), bf16),
            pltpu.VMEM((128, 128), f32),
            pltpu.VMEM((128, 128), f32),
        ],
        scratch_shapes=scratch_like(weights),
        cost_estimate=cost(2000000000, 4 << 20),
        compiler_params=pltpu.CompilerParams(vmem_limit_bytes=VMEM_LIMIT),
        name="row_side",
    )(x, *packs, *small, rate, *in_hbm(weights))


def readout_kernel(probe_ref, pv_ref, gate_ref, *rest):
    packs, states, out_ref = rest[:8], rest[8:16], rest[16]
    core = lax.rem(lax.axis_index("tp"), 2)
    own = iota((32, 16, 128), 0) == iota((32, 16, 128), 2) % 32
    pieces = []
    for state in states:
        block = state[pl.ds(pl.multiple_of(512 * core, 512), 512), :]
        read = dot(block, probe_ref[...], 1, 0)
        pieces.append(jnp.sum(jnp.where(own, read.reshape(32, 16, 128), 0.0), axis=0))
    o = jnp.concatenate(pieces, axis=0) + pv_ref[...]
    o = o * lax.rsqrt(jnp.mean(o * o, axis=0, keepdims=True) + epsilon)
    o = (o * gate_ref[...]).astype(bf16)
    out_ref[...] = dot(o, weight_rows(packs, 32), 0, 0).astype(bf16)


def readout(probe, pv, gate, packs, states):
    return pl.pallas_call(
        readout_kernel,
        in_specs=vmem_specs(19),
        out_specs=pl.BlockSpec(memory_space=pltpu.VMEM),
        out_shape=pltpu.VMEM((128, 2048), bf16),
        cost_estimate=cost(500000000, 3 << 20),
        compiler_params=pltpu.CompilerParams(vmem_limit_bytes=VMEM_LIMIT),
        name="readout",
    )(probe, pv, gate, *packs, *states)


def total_kernel(part_ref, out_ref):
    total = jnp.sum(part_ref[...].astype(f32), axis=0)
    total = total * lax.rsqrt(jnp.mean(total * total, axis=1, keepdims=True) + epsilon)
    stacked = jnp.concatenate([total[:, 128 * c : 128 * c + 128] for c in range(16)], axis=0)
    out_ref[...] = stacked.T


def sum_heads(parts):
    return pl.pallas_call(
        total_kernel,
        in_specs=vmem_specs(1),
        out_specs=pl.BlockSpec(memory_space=pltpu.VMEM),
        out_shape=pltpu.VMEM((128, 128), f32),
        cost_estimate=cost(1000000, 1 << 19),
        compiler_params=pltpu.CompilerParams(vmem_limit_bytes=VMEM_LIMIT),
        name="sum_heads",
    )(parts)


def final_kernel(x_ref, gain_ref, out_ref, scratch):
    place = iota((128, 16), 0) // 8 == iota((128, 16), 1)
    gain = jnp.sum(jnp.where(place, gain_ref[...].astype(f32), 0.0), axis=1, keepdims=True)
    scratch[...] = x_ref[...].T * gain
    lane = iota((1, 128), 1)
    rows = [scratch[pl.ds(r, 16, 8), :] for r in range(8)]
    blocks = []
    for i in range(4):
        halves = []
        for h in range(2):
            packed = None
            for q in range(4):
                shift = (32 * q - 32 * i) % 128
                moved = roll(rows[4 * h + q], shift) if shift else rows[4 * h + q]
                packed = moved if packed is None else jnp.where(lane // 32 == q, moved, packed)
            halves.append(packed)
        blocks.append(jnp.concatenate(halves, axis=1))
    full = jnp.concatenate(blocks, axis=0).astype(bf16)
    source = iota((256, 256), 0)
    target = iota((256, 256), 1)
    wanted = (source % 8) * 32 + ((source // 8) % 4) * 8 + source // 32
    order = jnp.where(wanted == target, 1.0, 0.0).astype(bf16)
    out_ref[...] = dot(full, order, 1, 0).astype(bf16).reshape(4, 16, 256)


def final_rows(x, gain):
    return pl.pallas_call(
        final_kernel,
        in_specs=vmem_specs(2),
        out_specs=pl.BlockSpec(memory_space=pltpu.VMEM),
        out_shape=jax.ShapeDtypeStruct((4, 16, 256), bf16),
        scratch_shapes=[pltpu.VMEM((128, 128), f32)],
        cost_estimate=cost(10000000, 1 << 18),
        compiler_params=pltpu.CompilerParams(vmem_limit_bytes=VMEM_LIMIT),
        name="final_rows",
    )(x, gain)


def chip_permute(x, d):
    return lax.ppermute(x, "tp", [((i + 2 * d) % 8, i) for i in range(8)])


def core_permute(x):
    return lax.ppermute(x, "tp", [(i ^ 1, i) for i in range(8)])


def whole_step(
    tokens,
    input_norm_gain,
    query_weight,
    key_weight,
    value_weight,
    output_gate_weight,
    strength_weight,
    decay_weight,
    head_decay_rate,
    proposal_log_decay,
    head_norm_gain,
    output_weight,
    output_norm_gain,
    state,
    previous_keys,
    previous_values,
    previous_log_decay,
    previous_strengths,
    accepted,
    parent,
):
    sent, pack, bundle, *ahead, other_rows = prepare(
        (
            jnp.transpose(tokens, (1, 2, 0)),
            jnp.transpose(value_weight[:, 0, :], (1, 0)),
            jnp.transpose(output_gate_weight[:, 0, :], (1, 0)),
            output_weight[0],
            head_norm_gain.reshape(1, 16),
        ),
        (
            previous_keys.reshape(1024, 128),
            jnp.transpose(previous_values[:, :, 0, :], (1, 2, 0)),
            jnp.transpose(previous_strengths, (1, 2, 0)),
            jnp.transpose(previous_log_decay, (1, 2, 0)),
            accepted.reshape(1, 256),
            input_norm_gain.reshape(16, 128),
            jnp.transpose(strength_weight, (1, 0)),
            jnp.transpose(decay_weight, (1, 0)),
            jnp.transpose(proposal_log_decay, (1, 2, 0)),
            jnp.transpose(parent, (1, 0)),
        ),
        state.reshape(256, 16, 128),
    )
    ahead, small = ahead[:5], ahead[5:]
    near = [pack, chip_permute(pack, 1), chip_permute(bundle, 2), chip_permute(pack, 3)]
    x = lax.all_to_all(sent.reshape(128, 16, 128), BOTH, 0, 0, tiled=True).reshape(2048, 128)
    lows = other_chips_state(other_rows, ahead)
    accepted_state, own_low = all_chips_state(state.reshape(256, 16, 128), previous_keys.reshape(1024, 128), ahead[1:])
    one, three = chip_permute(lows[1], 1), chip_permute(lows[0], 3)
    packs = near + [core_permute(x) for x in near]
    partner_low = core_permute(own_low)
    states = [own_low, one, near[2], three, partner_low, core_permute(one), packs[6], core_permute(three)]
    rows = row_side(x, packs, small, head_decay_rate.reshape(1, 1), query_weight, key_weight)
    part = readout(*rows, packs, states)
    parts = lax.all_to_all(part.reshape(16, 8, 2048), "kv", 0, 0, tiled=True)
    blocks = lax.all_to_all(sum_heads(parts), BOTH, 0, 0, tiled=True)
    out = final_rows(blocks, output_norm_gain.reshape(1, 16))
    return jnp.transpose(out, (2, 0, 1)), accepted_state.reshape(state.shape)


def solution(mesh):
    placed = (
        P(None, None, ("kv", "tp")),
        P(),
        P(None, "kv"),
        P(None, "kv"),
        P(None, "kv", "tp"),
        P(None, "kv", "tp"),
        P(None, "kv"),
        P(None, "kv"),
        P("kv"),
        P(None, None, "kv"),
        P("tp"),
        P("kv", "tp", None),
        P(("kv", "tp")),
        P(None, "kv", "tp", None),
        P(None, None, "kv"),
        P(None, None, "kv", "tp"),
        P(None, None, "kv"),
        P(None, None, "kv"),
        P(),
        P(),
    )
    return jax.shard_map(
        whole_step,
        mesh=mesh,
        in_specs=placed,
        out_specs=(P(None, None, ("kv", "tp")), P(None, "kv", "tp", None)),
        check_vma=False,
    )
```

```python
import jax
import jax.numpy as jnp
from jax import lax
from jax.experimental import pallas as pl
from jax.experimental.pallas import tpu as pltpu
from jax.sharding import PartitionSpec as P


epsilon = 1e-06
f32 = jnp.float32
bf16 = jnp.bfloat16
BOTH = ("kv", "tp")
VMEM_LIMIT = 16 << 20
PACK = 784
BUNDLE = 1024 + PACK


def dot(a, b, ca, cb):
    return lax.dot_general(a, b, (((ca,), (cb,)), ((), ())), preferred_element_type=f32)


def iota(shape, dim):
    return lax.broadcasted_iota(jnp.int32, shape, dim)


def roll(x, shift):
    return pltpu.roll(x, shift, 1)


def cost(flops, size):
    return pl.CostEstimate(flops=flops, bytes_accessed=size, transcendentals=0)


def chunk_lanes(rows, group):
    lane = iota((1, 128), 1)
    packed = None
    for j in range(4):
        if isinstance(group, int):
            half = rows[j][:, 128 * (group // 4) : 128 * (group // 4) + 128]
            shift = (32 * j - 32 * (group % 4)) % 128
            moved = roll(half, shift) if shift else half
        else:
            half = jnp.where(group >= 4, rows[j][:, 128:], rows[j][:, :128])
            moved = roll(half, lax.rem(32 * j + 128 - 32 * lax.rem(group, 4), 128))
        packed = moved if packed is None else jnp.where(lane // 32 == j, moved, packed)
    return packed


def solve(rhs, coupling):
    x = rhs
    for _ in range(3):
        x = rhs - sum(coupling[d] * roll(x, 32 * d) for d in (1, 2, 3))
    return x


def hbm_specs(count):
    return [pl.BlockSpec(memory_space=pltpu.HBM)] * count


def vmem_specs(count):
    return [pl.BlockSpec(memory_space=pltpu.VMEM)] * count


def start_all(copies):
    for copy in copies:
        copy.start()


def wait_all(copies):
    for copy in copies:
        copy.wait()


def copies_in(sources, targets, sems):
    return [pltpu.make_async_copy(x, y, sems.at[i]) for i, (x, y) in enumerate(zip(sources, targets))]


def in_hbm(arrays):
    return [pltpu.with_memory_space_constraint(x, pltpu.HBM) for x in arrays]


def scratch_like(arrays):
    return [pltpu.VMEM(x.shape, x.dtype) for x in arrays] + [pltpu.SemaphoreType.DMA((len(arrays),))]


def prepare_kernel(*refs):
    sources, state_source, (sent_out, pack_ref, bundle_ref), kept, rest = (
        refs[:15], refs[15], refs[16:19], refs[19:29], refs[29:],
    )
    low_ref, held, sems, state_ref, sent_ref, sent_sem = rest[0], rest[1:6], rest[6:9], rest[9], rest[10], rest[11]
    copies = copies_in(sources[:5], held, sems[0])
    ahead = copies_in(sources[5:], kept, sems[1])
    chip = lax.axis_index("tp") // 2
    loads = []
    for i, offset in enumerate((2, 1, 3)):
        rows = pl.ds(pl.multiple_of(64 * lax.rem(chip + offset, 4), 64), 64)
        loads.append(pltpu.make_async_copy(state_source.at[rows], state_ref.at[pl.ds(64 * i, 64)], sems[2].at[i]))
    start_all(copies[:1] + loads[:1] + ahead[:5] + copies[1:] + loads[1:] + ahead[5:])
    copies[0].wait()
    rows = [held[0][i].astype(f32) for i in range(4)]
    for t in range(8):
        block = chunk_lanes(rows, t).astype(bf16)
        for k in range(16):
            sent_ref[k, t] = block
    send = pltpu.make_async_copy(sent_ref, sent_out, sent_sem)
    send.start()
    wait_all(copies[1:])
    pack_weights(*held[1:], pack_ref)
    bundle_ref[1024:, :] = pack_ref[...]
    wait_all(ahead[:5] + loads[:1])

    def read(step):
        return state_ref[32 * step : 32 * step + 32].reshape(512, 128)

    def emit(step, new):
        bundle_ref[512 * step : 512 * step + 512, :] = new.astype(bf16)

    state_update((2,), kept[:5], read, emit)
    wait_all(loads[1:])
    for i in range(4):
        low_ref[512 * i : 512 * i + 512, :] = read(2 + i).astype(bf16)
    wait_all(ahead[5:] + [send])


def prepare(first, ahead, state):
    return pl.pallas_call(
        prepare_kernel,
        in_specs=hbm_specs(16),
        out_specs=hbm_specs(1) + vmem_specs(13),
        out_shape=[pltpu.HBM((16, 8, 16, 128), bf16), pltpu.VMEM((PACK, 128), bf16), pltpu.VMEM((BUNDLE, 128), bf16)]
        + [pltpu.VMEM(x.shape, x.dtype) for x in ahead]
        + [pltpu.VMEM((2048, 128), bf16)],
        scratch_shapes=scratch_like(first)
        + [pltpu.SemaphoreType.DMA((10,)), pltpu.SemaphoreType.DMA((3,)), pltpu.VMEM((192, 16, 128), f32)]
        + [pltpu.VMEM((16, 8, 16, 128), bf16), pltpu.SemaphoreType.DMA],
        cost_estimate=cost(10000000, 1 << 20),
        compiler_params=pltpu.CompilerParams(vmem_limit_bytes=VMEM_LIMIT),
        name="prepare",
    )(*in_hbm((*first, *ahead, state)))


def stack(rows):
    return jnp.concatenate(rows, axis=0)


def spread_rows(x):
    count = x.shape[0]
    return jnp.broadcast_to(x[:, None, :], (count, 16, 128)).reshape(16 * count, 128)


def state_update(chips, operands, read, emit):
    key_ref, value_ref, strength_ref, decay_ref, accepted_ref = operands
    steps = range(2 * len(chips))
    chip = lax.axis_index("tp") // 2
    groups = [2 * lax.rem(chip + chips[step // 2], 4) + step % 2 for step in steps]
    lane = iota((1, 128), 1)
    place = lane // 32
    strength = stack([chunk_lanes([strength_ref[j] for j in range(4)], x) for x in groups])
    decay = stack([chunk_lanes([decay_ref[j] for j in range(4)], x) for x in groups])
    accepted = stack([chunk_lanes([accepted_ref[...].astype(f32)] * 4, x) for x in groups])
    values = [value_ref[j].astype(f32) for j in range(4)]
    values = stack([chunk_lanes(values, x) for x in groups])
    live = jnp.where(place < accepted, 1.0, 0.0)
    beta = strength * live
    g = decay * live
    gam = g + sum(jnp.where(place >= d, roll(g, 32 * d), 0.0) for d in (1, 2, 3))
    last = g + sum(roll(g, 32 * d) for d in (1, 2, 3))
    row = iota((128, 128), 0)
    column = iota((128, 128), 1)
    order = jnp.where(column == (row % 32) * 4 + row // 32, 1.0, 0.0).astype(bf16)
    keys = [dot(order, key_ref[pl.ds(pl.multiple_of(128 * x, 128), 128), :], 1, 0).astype(bf16) for x in groups]
    grams = [dot(x, x, 1, 1) for x in keys]

    def diagonal(d):
        return stack(
            [jnp.sum(jnp.where(row == column - 32 * d, gram, 0.0), axis=0, keepdims=True) for gram in grams]
        )

    unit = lax.rsqrt(diagonal(0) + epsilon)
    coupling = {
        d: jnp.where(
            place >= d,
            beta * diagonal(d) * unit * roll(unit, 32 * d) * jnp.exp(jnp.minimum(gam - roll(gam, 32 * d), 0.0)),
            0.0,
        )
        for d in (1, 2, 3)
    }
    coupling = {d: spread_rows(x) for d, x in coupling.items()}
    own = iota((32, 16, 128), 0) == iota((32, 16, 128), 2) % 32
    seen = []
    for step in steps:
        product = dot(read(step).astype(bf16), keys[step], 1, 1)
        seen.append(jnp.sum(jnp.where(own, product.reshape(32, 16, 128), 0.0), axis=0))
    update = solve(spread_rows(beta) * values - spread_rows(beta * jnp.exp(gam) * unit) * stack(seen), coupling)
    update = update * spread_rows(jnp.exp(last - gam) * unit)
    keep = jnp.exp(last)
    for step in steps:
        spread = jnp.broadcast_to(update[16 * step : 16 * step + 16][None], (32, 16, 128))
        change = dot(jnp.where(own, spread, 0.0).reshape(512, 128).astype(bf16), keys[step], 1, 0)
        kept = jnp.where(iota((32, 128), 0) == iota((32, 128), 1), keep[step : step + 1], 0.0)
        kept = jnp.broadcast_to(jnp.sum(kept, axis=1, keepdims=True), (32, 128))
        kept = jnp.broadcast_to(kept[:, None, :], (32, 16, 128))
        emit(step, kept.reshape(512, 128) * read(step).astype(f32) + change)


def other_chips_kernel(state_ref, *refs):
    operands, lows = refs[:5], refs[5:]

    def emit(step, new):
        lows[step // 2][512 * (step % 2) : 512 * (step % 2) + 512, :] = new.astype(bf16)

    state_update((1, 3), operands, lambda step: state_ref[512 * step : 512 * step + 512, :], emit)


def other_chips_state(state, operands):
    return pl.pallas_call(
        other_chips_kernel,
        in_specs=vmem_specs(6),
        out_specs=vmem_specs(2),
        out_shape=[pltpu.VMEM((1024, 128), bf16)] * 2,
        cost_estimate=cost(1000000000, 2 << 20),
        compiler_params=pltpu.CompilerParams(vmem_limit_bytes=VMEM_LIMIT),
        name="other_chips_state",
    )(state, *operands)


def all_chips_kernel(source, key_source, *refs):
    operands, (state_out, low_ref, state_ref, key_ref, sems) = refs[:4], refs[4:]
    chip = lax.axis_index("tp") // 2

    def rows_of(i):
        return pl.ds(pl.multiple_of(64 * lax.rem(chip + i, 4), 64), 64)

    def held(i):
        return pl.ds(64 * i, 64)

    loads = [pltpu.make_async_copy(source.at[rows_of(i)], state_ref.at[held(i)], sems.at[0, i]) for i in range(4)]
    stores = [pltpu.make_async_copy(state_ref.at[held(i)], state_out.at[rows_of(i)], sems.at[1, i]) for i in range(4)]
    keys = pltpu.make_async_copy(key_source, key_ref, sems.at[0, 4])
    keys.start()
    start_all(loads)
    keys.wait()
    arrived = set()

    def read(step):
        if step // 2 not in arrived:
            arrived.add(step // 2)
            loads[step // 2].wait()
        return state_ref[32 * step : 32 * step + 32].reshape(512, 128)

    def emit(step, new):
        state_ref[32 * step : 32 * step + 32] = new.reshape(32, 16, 128)
        if step < 2:
            low_ref[512 * step : 512 * step + 512, :] = new.astype(bf16)
        if step % 2 == 1:
            stores[step // 2].start()

    state_update((0, 1, 2, 3), (key_ref, *operands), read, emit)
    wait_all(stores)


def all_chips_state(state, keys, operands):
    return pl.pallas_call(
        all_chips_kernel,
        in_specs=hbm_specs(2) + vmem_specs(4),
        out_specs=hbm_specs(1) + vmem_specs(1),
        out_shape=[pltpu.HBM((256, 16, 128), f32), pltpu.VMEM((1024, 128), bf16)],
        scratch_shapes=[
            pltpu.VMEM((256, 16, 128), f32),
            pltpu.VMEM((1024, 128), bf16),
            pltpu.SemaphoreType.DMA((2, 5)),
        ],
        cost_estimate=cost(2000000000, 4 << 20),
        compiler_params=pltpu.CompilerParams(vmem_limit_bytes=VMEM_LIMIT),
        name="all_chips_state",
    )(*in_hbm((state, keys)), *operands)


def pack_weights(value_ref, gate_ref, output_ref, gain_ref, pack_ref):
    row = iota((16, 16), 0)
    gain = jnp.where(row == iota((16, 16), 1), jnp.broadcast_to(gain_ref[...].astype(f32), (16, 16)), 0.0)
    gain = jnp.broadcast_to(jnp.sum(gain, axis=1, keepdims=True), (16, 128)).astype(bf16)
    source = iota((128, 128), 0)
    target = iota((128, 128), 1)
    order = jnp.where(target == (source % 16) * 8 + source // 16, 1.0, 0.0).astype(bf16)
    rows = jnp.concatenate([output_ref[:, 128 * b : 128 * b + 128] for b in range(16)], axis=0)
    rows = dot(rows, order, 1, 0)
    lane = iota((1, 128), 1)
    for c in range(16):
        packed = None
        for b in range(16):
            piece = rows[16 * b : 16 * b + 16, :]
            shift = (8 * (b - c)) % 128
            moved = roll(piece, shift) if shift else piece
            packed = moved if packed is None else jnp.where(lane // 8 == b, moved, packed)
        columns = slice(128 * c, 128 * c + 128)
        block = jnp.concatenate([value_ref[:, columns], gate_ref[:, columns], packed.astype(bf16)], axis=0)
        pack_ref[48 * c : 48 * c + 48, :] = block
    pack_ref[768:, :] = gain


def pack_rows(ref, first, count):
    base = ref.shape[0] - PACK
    return ref[base + first : base + first + count, :]


def weight_rows(packs, first):
    return jnp.concatenate(
        [stack([pack_rows(x, 48 * b + first, 16) for x in packs]) for b in range(16)],
        axis=1,
    )


def rows_kernel(x_ref, *refs):
    packs, small, rate_ref, sources, outs, held, sems = (
        refs[:8], refs[8:13], refs[13], refs[14:16], refs[16:19], refs[19:21], refs[21],
    )
    gain_ref, strength_ref, decay_ref, log_decay_ref, parent_ref = small
    probe_ref, pv_ref, gate_ref = outs
    wq_ref, wk_ref = held
    copies = copies_in(sources, held, sems)
    start_all(copies)
    group = lax.axis_index("tp")
    x = x_ref[...].astype(f32)
    scale = lax.rsqrt(jnp.mean(x * x, axis=0, keepdims=True) + epsilon)
    column = iota((128, 128), 1) == iota((128, 128), 0)
    gain = jnp.concatenate(
        [jnp.where(column, gain_ref[b : b + 1, :].astype(f32), 0.0).astype(bf16) for b in range(16)], axis=0
    )
    gain = dot(gain, jnp.ones((128, 128), bf16), 1, 0)
    normed = (x * scale * gain).astype(bf16)

    def project(weight, dim):
        return dot(weight, normed, dim, 0)

    def rounded(x):
        return x.astype(bf16).astype(f32)

    first = iota((16, 2048), 0) == 0
    scalars = jnp.where(first, strength_ref[...].astype(f32), decay_ref[...].astype(f32))
    scalars = scalars.astype(bf16)
    both = jnp.concatenate([weight_rows(packs, 0), weight_rows(packs, 16)], axis=0)
    both = rounded(project(both, 1))
    values, zgate = both[:128], both[128:]
    logits = project(scalars, 1)
    wait_all(copies)
    queries = rounded(project(wq_ref[...], 0))
    keys = rounded(project(wk_ref[...], 0))
    gain = jnp.concatenate([pack_rows(pack, 768, 16) for pack in packs], axis=0).astype(f32)

    def unit(x):
        return x * lax.rsqrt(jnp.sum(x * x, axis=0, keepdims=True) + epsilon)

    queries = unit(queries) * 128**-0.5
    keys = unit(keys)
    beta = jax.nn.sigmoid(logits[0:1, :])
    pre = logits[1:2, :]
    softplus = jnp.maximum(pre, 0.0) + jnp.log1p(jnp.exp(-jnp.abs(pre)))
    log_decay = chunk_lanes([log_decay_ref[i] for i in range(4)], group)
    parent = chunk_lanes([parent_ref[i : i + 1, :].astype(f32) for i in range(4)], group)
    g = log_decay - rate_ref[0, 0] * softplus
    place = (iota((1, 128), 1) // 32).astype(f32)
    hit = {d: jnp.where((parent == place - d) & (place >= d), 1.0, 0.0) for d in (1, 2, 3)}
    seen = {1: hit[1]}
    seen[2] = hit[2] + hit[1] * roll(seen[1], 32)
    seen[3] = hit[3] + hit[1] * roll(seen[2], 32) + hit[2] * roll(seen[1], 64)
    gam = g + sum(seen[d] * roll(g, 32 * d) for d in (1, 2, 3))
    coupling, reach = {}, {0: jnp.sum(queries * keys, axis=0, keepdims=True)}
    for d in (1, 2, 3):
        earlier = roll(keys, 32 * d)
        weight = jnp.exp(jnp.minimum(gam - roll(gam, 32 * d), 0.0)) * seen[d]
        coupling[d] = beta * weight * jnp.sum(keys * earlier, axis=0, keepdims=True)
        reach[d] = weight * jnp.sum(queries * earlier, axis=0, keepdims=True)
    solved_values = solve(beta * values, coupling)
    solved_keys = solve((beta * jnp.exp(gam)) * keys, coupling)

    def reached(x):
        return reach[0] * x + sum(reach[d] * roll(x, 32 * d) for d in (1, 2, 3))

    probe = jnp.exp(gam) * queries - reached(solved_keys)
    probe_ref[...] = probe.astype(bf16)
    pv_ref[...] = reached(solved_values)
    gate_ref[...] = gain * (zgate * jax.nn.sigmoid(zgate))


def row_side(x, packs, small, rate, *weights):
    return pl.pallas_call(
        rows_kernel,
        in_specs=vmem_specs(14) + [pl.BlockSpec(memory_space=pltpu.SMEM)] + hbm_specs(2),
        out_specs=vmem_specs(3),
        out_shape=[
            pltpu.VMEM((128, 128), bf16),
            pltpu.VMEM((128, 128), f32),
            pltpu.VMEM((128, 128), f32),
        ],
        scratch_shapes=scratch_like(weights),
        cost_estimate=cost(2000000000, 4 << 20),
        compiler_params=pltpu.CompilerParams(vmem_limit_bytes=VMEM_LIMIT),
        name="row_side",
    )(x, *packs, *small, rate, *in_hbm(weights))


def readout_kernel(probe_ref, pv_ref, gate_ref, *rest):
    packs, states, out_ref = rest[:8], rest[8:16], rest[16]
    core = lax.rem(lax.axis_index("tp"), 2)
    own = iota((32, 16, 128), 0) == iota((32, 16, 128), 2) % 32
    pieces = []
    for state in states:
        block = state[pl.ds(pl.multiple_of(512 * core, 512), 512), :]
        read = dot(block, probe_ref[...], 1, 0)
        pieces.append(jnp.sum(jnp.where(own, read.reshape(32, 16, 128), 0.0), axis=0))
    o = jnp.concatenate(pieces, axis=0) + pv_ref[...]
    o = o * lax.rsqrt(jnp.mean(o * o, axis=0, keepdims=True) + epsilon)
    o = (o * gate_ref[...]).astype(bf16)
    out_ref[...] = dot(o, weight_rows(packs, 32), 0, 0).astype(bf16)


def readout(probe, pv, gate, packs, states):
    return pl.pallas_call(
        readout_kernel,
        in_specs=vmem_specs(19),
        out_specs=pl.BlockSpec(memory_space=pltpu.VMEM),
        out_shape=pltpu.VMEM((128, 2048), bf16),
        cost_estimate=cost(500000000, 3 << 20),
        compiler_params=pltpu.CompilerParams(vmem_limit_bytes=VMEM_LIMIT),
        name="readout",
    )(probe, pv, gate, *packs, *states)


def total_kernel(part_ref, out_ref):
    total = jnp.sum(part_ref[...].astype(f32), axis=0)
    total = total * lax.rsqrt(jnp.mean(total * total, axis=1, keepdims=True) + epsilon)
    stacked = jnp.concatenate([total[:, 128 * c : 128 * c + 128] for c in range(16)], axis=0)
    out_ref[...] = stacked.T


def sum_heads(parts):
    return pl.pallas_call(
        total_kernel,
        in_specs=vmem_specs(1),
        out_specs=pl.BlockSpec(memory_space=pltpu.VMEM),
        out_shape=pltpu.VMEM((128, 128), f32),
        cost_estimate=cost(1000000, 1 << 19),
        compiler_params=pltpu.CompilerParams(vmem_limit_bytes=VMEM_LIMIT),
        name="sum_heads",
    )(parts)


def final_kernel(x_ref, gain_ref, out_ref, scratch):
    place = iota((128, 16), 0) // 8 == iota((128, 16), 1)
    gain = jnp.sum(jnp.where(place, gain_ref[...].astype(f32), 0.0), axis=1, keepdims=True)
    scratch[...] = x_ref[...].T * gain
    lane = iota((1, 128), 1)
    rows = [scratch[pl.ds(r, 16, 8), :] for r in range(8)]
    blocks = []
    for i in range(4):
        halves = []
        for h in range(2):
            packed = None
            for q in range(4):
                shift = (32 * q - 32 * i) % 128
                moved = roll(rows[4 * h + q], shift) if shift else rows[4 * h + q]
                packed = moved if packed is None else jnp.where(lane // 32 == q, moved, packed)
            halves.append(packed)
        blocks.append(jnp.concatenate(halves, axis=1))
    full = jnp.concatenate(blocks, axis=0).astype(bf16)
    source = iota((256, 256), 0)
    target = iota((256, 256), 1)
    wanted = (source % 8) * 32 + ((source // 8) % 4) * 8 + source // 32
    order = jnp.where(wanted == target, 1.0, 0.0).astype(bf16)
    out_ref[...] = dot(full, order, 1, 0).astype(bf16).reshape(4, 16, 256)


def final_rows(x, gain):
    return pl.pallas_call(
        final_kernel,
        in_specs=vmem_specs(2),
        out_specs=pl.BlockSpec(memory_space=pltpu.VMEM),
        out_shape=jax.ShapeDtypeStruct((4, 16, 256), bf16),
        scratch_shapes=[pltpu.VMEM((128, 128), f32)],
        cost_estimate=cost(10000000, 1 << 18),
        compiler_params=pltpu.CompilerParams(vmem_limit_bytes=VMEM_LIMIT),
        name="final_rows",
    )(x, gain)


def chip_permute(x, d):
    return lax.ppermute(x, "tp", [((i + 2 * d) % 8, i) for i in range(8)])


def core_permute(x):
    return lax.ppermute(x, "tp", [(i ^ 1, i) for i in range(8)])


def whole_step(
    tokens,
    input_norm_gain,
    query_weight,
    key_weight,
    value_weight,
    output_gate_weight,
    strength_weight,
    decay_weight,
    head_decay_rate,
    proposal_log_decay,
    head_norm_gain,
    output_weight,
    output_norm_gain,
    state,
    previous_keys,
    previous_values,
    previous_log_decay,
    previous_strengths,
    accepted,
    parent,
):
    sent, pack, bundle, *ahead, other_rows = prepare(
        (
            jnp.transpose(tokens, (1, 2, 0)),
            jnp.transpose(value_weight[:, 0, :], (1, 0)),
            jnp.transpose(output_gate_weight[:, 0, :], (1, 0)),
            output_weight[0],
            head_norm_gain.reshape(1, 16),
        ),
        (
            previous_keys.reshape(1024, 128),
            jnp.transpose(previous_values[:, :, 0, :], (1, 2, 0)),
            jnp.transpose(previous_strengths, (1, 2, 0)),
            jnp.transpose(previous_log_decay, (1, 2, 0)),
            accepted.reshape(1, 256),
            input_norm_gain.reshape(16, 128),
            jnp.transpose(strength_weight, (1, 0)),
            jnp.transpose(decay_weight, (1, 0)),
            jnp.transpose(proposal_log_decay, (1, 2, 0)),
            jnp.transpose(parent, (1, 0)),
        ),
        state.reshape(256, 16, 128),
    )
    ahead, small = ahead[:5], ahead[5:]
    near = [pack, chip_permute(pack, 1), chip_permute(bundle, 2), chip_permute(pack, 3)]
    x = lax.all_to_all(sent.reshape(128, 16, 128), BOTH, 0, 0, tiled=True).reshape(2048, 128)
    lows = other_chips_state(other_rows, ahead)
    accepted_state, own_low = all_chips_state(state.reshape(256, 16, 128), previous_keys.reshape(1024, 128), ahead[1:])
    one, three = chip_permute(lows[1], 1), chip_permute(lows[0], 3)
    packs = near + [core_permute(x) for x in near]
    partner_low = core_permute(own_low)
    states = [own_low, one, near[2], three, partner_low, core_permute(one), packs[6], core_permute(three)]
    rows = row_side(x, packs, small, head_decay_rate.reshape(1, 1), query_weight, key_weight)
    part = readout(*rows, packs, states)
    parts = lax.all_to_all(part.reshape(16, 8, 2048), "kv", 0, 0, tiled=True)
    blocks = lax.all_to_all(sum_heads(parts), BOTH, 0, 0, tiled=True)
    out = final_rows(blocks, output_norm_gain.reshape(1, 16))
    return jnp.transpose(out, (2, 0, 1)), accepted_state.reshape(state.shape)


def solution(mesh):
    placed = (
        P(None, None, ("kv", "tp")),
        P(),
        P(None, "kv"),
        P(None, "kv"),
        P(None, "kv", "tp"),
        P(None, "kv", "tp"),
        P(None, "kv"),
        P(None, "kv"),
        P("kv"),
        P(None, None, "kv"),
        P("tp"),
        P("kv", "tp", None),
        P(("kv", "tp")),
        P(None, "kv", "tp", None),
        P(None, None, "kv"),
        P(None, None, "kv", "tp"),
        P(None, None, "kv"),
        P(None, None, "kv"),
        P(),
        P(),
    )
    return jax.shard_map(
        whole_step,
        mesh=mesh,
        in_specs=placed,
        out_specs=(P(None, None, ("kv", "tp")), P(None, "kv", "tp", None)),
        check_vma=False,
    )
```

```python
import jax
import jax.numpy as jnp
from jax import lax
from jax.experimental import pallas as pl
from jax.experimental.pallas import tpu as pltpu
from jax.sharding import PartitionSpec as P


epsilon = 1e-06
f32 = jnp.float32
bf16 = jnp.bfloat16
BOTH = ("kv", "tp")
VMEM_LIMIT = 16 << 20
PACK = 784
BUNDLE = 1024 + PACK


def dot(a, b, ca, cb):
    return lax.dot_general(a, b, (((ca,), (cb,)), ((), ())), preferred_element_type=f32)


def iota(shape, dim):
    return lax.broadcasted_iota(jnp.int32, shape, dim)


def roll(x, shift):
    return pltpu.roll(x, shift, 1)


def cost(flops, size):
    return pl.CostEstimate(flops=flops, bytes_accessed=size, transcendentals=0)


def chunk_lanes(rows, group):
    lane = iota((1, 128), 1)
    packed = None
    for j in range(4):
        if isinstance(group, int):
            half = rows[j][:, 128 * (group // 4) : 128 * (group // 4) + 128]
            shift = (32 * j - 32 * (group % 4)) % 128
            moved = roll(half, shift) if shift else half
        else:
            half = jnp.where(group >= 4, rows[j][:, 128:], rows[j][:, :128])
            moved = roll(half, lax.rem(32 * j + 128 - 32 * lax.rem(group, 4), 128))
        packed = moved if packed is None else jnp.where(lane // 32 == j, moved, packed)
    return packed


def solve(rhs, coupling):
    x = rhs
    for _ in range(3):
        x = rhs - sum(coupling[d] * roll(x, 32 * d) for d in (1, 2, 3))
    return x


def hbm_specs(count):
    return [pl.BlockSpec(memory_space=pltpu.HBM)] * count


def vmem_specs(count):
    return [pl.BlockSpec(memory_space=pltpu.VMEM)] * count


def start_all(copies):
    for copy in copies:
        copy.start()


def wait_all(copies):
    for copy in copies:
        copy.wait()


def copies_in(sources, targets, sems):
    return [pltpu.make_async_copy(x, y, sems.at[i]) for i, (x, y) in enumerate(zip(sources, targets))]


def in_hbm(arrays):
    return [pltpu.with_memory_space_constraint(x, pltpu.HBM) for x in arrays]


def scratch_like(arrays):
    return [pltpu.VMEM(x.shape, x.dtype) for x in arrays] + [pltpu.SemaphoreType.DMA((len(arrays),))]


def prepare_kernel(*refs):
    sources, state_source, (sent_out, pack_ref, bundle_ref), kept, rest = (
        refs[:15], refs[15], refs[16:19], refs[19:29], refs[29:],
    )
    low_ref, held, sems, state_ref, sent_ref, sent_sem = rest[0], rest[1:6], rest[6:9], rest[9], rest[10], rest[11]
    copies = copies_in(sources[:5], held, sems[0])
    ahead = copies_in(sources[5:], kept, sems[1])
    chip = lax.axis_index("tp") // 2
    loads = []
    for i, offset in enumerate((2, 1, 3)):
        rows = pl.ds(pl.multiple_of(64 * lax.rem(chip + offset, 4), 64), 64)
        loads.append(pltpu.make_async_copy(state_source.at[rows], state_ref.at[pl.ds(64 * i, 64)], sems[2].at[i]))
    start_all(copies[:1] + loads[:1] + ahead[:5] + copies[1:] + loads[1:] + ahead[5:])
    copies[0].wait()
    rows = [held[0][i].astype(f32) for i in range(4)]
    for t in range(8):
        block = chunk_lanes(rows, t).astype(bf16)
        for k in range(16):
            sent_ref[k, t] = block
    send = pltpu.make_async_copy(sent_ref, sent_out, sent_sem)
    send.start()
    wait_all(copies[1:])
    pack_weights(*held[1:], pack_ref)
    bundle_ref[1024:, :] = pack_ref[...]
    wait_all(ahead[:5] + loads[:1])

    def read(step):
        return state_ref[32 * step : 32 * step + 32].reshape(512, 128)

    def emit(step, new):
        bundle_ref[512 * step : 512 * step + 512, :] = new.astype(bf16)

    state_update((2,), kept[:5], read, emit)
    wait_all(loads[1:])
    for i in range(4):
        low_ref[512 * i : 512 * i + 512, :] = read(2 + i).astype(bf16)
    wait_all(ahead[5:] + [send])


def prepare(first, ahead, state):
    return pl.pallas_call(
        prepare_kernel,
        in_specs=hbm_specs(16),
        out_specs=hbm_specs(1) + vmem_specs(13),
        out_shape=[pltpu.HBM((16, 8, 16, 128), bf16), pltpu.VMEM((PACK, 128), bf16), pltpu.VMEM((BUNDLE, 128), bf16)]
        + [pltpu.VMEM(x.shape, x.dtype) for x in ahead]
        + [pltpu.VMEM((2048, 128), bf16)],
        scratch_shapes=scratch_like(first)
        + [pltpu.SemaphoreType.DMA((10,)), pltpu.SemaphoreType.DMA((3,)), pltpu.VMEM((192, 16, 128), f32)]
        + [pltpu.VMEM((16, 8, 16, 128), bf16), pltpu.SemaphoreType.DMA],
        cost_estimate=cost(10000000, 1 << 20),
        compiler_params=pltpu.CompilerParams(vmem_limit_bytes=VMEM_LIMIT),
        name="prepare",
    )(*in_hbm((*first, *ahead, state)))


def stack(rows):
    return jnp.concatenate(rows, axis=0)


def spread_rows(x):
    count = x.shape[0]
    return jnp.broadcast_to(x[:, None, :], (count, 16, 128)).reshape(16 * count, 128)


def state_update(chips, operands, read, emit):
    key_ref, value_ref, strength_ref, decay_ref, accepted_ref = operands
    steps = range(2 * len(chips))
    chip = lax.axis_index("tp") // 2
    groups = [2 * lax.rem(chip + chips[step // 2], 4) + step % 2 for step in steps]
    lane = iota((1, 128), 1)
    place = lane // 32
    strength = stack([chunk_lanes([strength_ref[j] for j in range(4)], x) for x in groups])
    decay = stack([chunk_lanes([decay_ref[j] for j in range(4)], x) for x in groups])
    accepted = stack([chunk_lanes([accepted_ref[...].astype(f32)] * 4, x) for x in groups])
    values = [value_ref[j].astype(f32) for j in range(4)]
    values = stack([chunk_lanes(values, x) for x in groups])
    live = jnp.where(place < accepted, 1.0, 0.0)
    beta = strength * live
    g = decay * live
    gam = g + sum(jnp.where(place >= d, roll(g, 32 * d), 0.0) for d in (1, 2, 3))
    last = g + sum(roll(g, 32 * d) for d in (1, 2, 3))
    row = iota((128, 128), 0)
    column = iota((128, 128), 1)
    order = jnp.where(column == (row % 32) * 4 + row // 32, 1.0, 0.0).astype(bf16)
    keys = [dot(order, key_ref[pl.ds(pl.multiple_of(128 * x, 128), 128), :], 1, 0).astype(bf16) for x in groups]
    grams = [dot(x, x, 1, 1) for x in keys]

    def diagonal(d):
        return stack(
            [jnp.sum(jnp.where(row == column - 32 * d, gram, 0.0), axis=0, keepdims=True) for gram in grams]
        )

    unit = lax.rsqrt(diagonal(0) + epsilon)
    coupling = {
        d: jnp.where(
            place >= d,
            beta * diagonal(d) * unit * roll(unit, 32 * d) * jnp.exp(jnp.minimum(gam - roll(gam, 32 * d), 0.0)),
            0.0,
        )
        for d in (1, 2, 3)
    }
    coupling = {d: spread_rows(x) for d, x in coupling.items()}
    own = iota((32, 16, 128), 0) == iota((32, 16, 128), 2) % 32
    seen = []
    for step in steps:
        product = dot(read(step).astype(bf16), keys[step], 1, 1)
        seen.append(jnp.sum(jnp.where(own, product.reshape(32, 16, 128), 0.0), axis=0))
    update = solve(spread_rows(beta) * values - spread_rows(beta * jnp.exp(gam) * unit) * stack(seen), coupling)
    update = update * spread_rows(jnp.exp(last - gam) * unit)
    keep = jnp.exp(last)
    for step in steps:
        spread = jnp.broadcast_to(update[16 * step : 16 * step + 16][None], (32, 16, 128))
        change = dot(jnp.where(own, spread, 0.0).reshape(512, 128).astype(bf16), keys[step], 1, 0)
        kept = jnp.where(iota((32, 128), 0) == iota((32, 128), 1), keep[step : step + 1], 0.0)
        kept = jnp.broadcast_to(jnp.sum(kept, axis=1, keepdims=True), (32, 128))
        kept = jnp.broadcast_to(kept[:, None, :], (32, 16, 128))
        emit(step, kept.reshape(512, 128) * read(step).astype(f32) + change)


def other_chips_kernel(state_ref, *refs):
    operands, lows = refs[:5], refs[5:]

    def emit(step, new):
        lows[step // 2][512 * (step % 2) : 512 * (step % 2) + 512, :] = new.astype(bf16)

    state_update((1, 3), operands, lambda step: state_ref[512 * step : 512 * step + 512, :], emit)


def other_chips_state(state, operands):
    return pl.pallas_call(
        other_chips_kernel,
        in_specs=vmem_specs(6),
        out_specs=vmem_specs(2),
        out_shape=[pltpu.VMEM((1024, 128), bf16)] * 2,
        cost_estimate=cost(1000000000, 2 << 20),
        compiler_params=pltpu.CompilerParams(vmem_limit_bytes=VMEM_LIMIT),
        name="other_chips_state",
    )(state, *operands)


def all_chips_kernel(source, key_source, *refs):
    operands, (state_out, low_ref, state_ref, key_ref, sems) = refs[:4], refs[4:]
    chip = lax.axis_index("tp") // 2

    def rows_of(i):
        return pl.ds(pl.multiple_of(64 * lax.rem(chip + i, 4), 64), 64)

    def held(i):
        return pl.ds(64 * i, 64)

    loads = [pltpu.make_async_copy(source.at[rows_of(i)], state_ref.at[held(i)], sems.at[0, i]) for i in range(4)]
    stores = [pltpu.make_async_copy(state_ref.at[held(i)], state_out.at[rows_of(i)], sems.at[1, i]) for i in range(4)]
    keys = pltpu.make_async_copy(key_source, key_ref, sems.at[0, 4])
    keys.start()
    start_all(loads)
    keys.wait()
    arrived = set()

    def read(step):
        if step // 2 not in arrived:
            arrived.add(step // 2)
            loads[step // 2].wait()
        return state_ref[32 * step : 32 * step + 32].reshape(512, 128)

    def emit(step, new):
        state_ref[32 * step : 32 * step + 32] = new.reshape(32, 16, 128)
        if step < 2:
            low_ref[512 * step : 512 * step + 512, :] = new.astype(bf16)
        if step % 2 == 1:
            stores[step // 2].start()

    state_update((0, 1, 2, 3), (key_ref, *operands), read, emit)
    wait_all(stores)


def all_chips_state(state, keys, operands):
    return pl.pallas_call(
        all_chips_kernel,
        in_specs=hbm_specs(2) + vmem_specs(4),
        out_specs=hbm_specs(1) + vmem_specs(1),
        out_shape=[pltpu.HBM((256, 16, 128), f32), pltpu.VMEM((1024, 128), bf16)],
        scratch_shapes=[
            pltpu.VMEM((256, 16, 128), f32),
            pltpu.VMEM((1024, 128), bf16),
            pltpu.SemaphoreType.DMA((2, 5)),
        ],
        cost_estimate=cost(2000000000, 4 << 20),
        compiler_params=pltpu.CompilerParams(vmem_limit_bytes=VMEM_LIMIT),
        name="all_chips_state",
    )(*in_hbm((state, keys)), *operands)


def pack_weights(value_ref, gate_ref, output_ref, gain_ref, pack_ref):
    row = iota((16, 16), 0)
    gain = jnp.where(row == iota((16, 16), 1), jnp.broadcast_to(gain_ref[...].astype(f32), (16, 16)), 0.0)
    gain = jnp.broadcast_to(jnp.sum(gain, axis=1, keepdims=True), (16, 128)).astype(bf16)
    source = iota((128, 128), 0)
    target = iota((128, 128), 1)
    order = jnp.where(target == (source % 16) * 8 + source // 16, 1.0, 0.0).astype(bf16)
    rows = jnp.concatenate([output_ref[:, 128 * b : 128 * b + 128] for b in range(16)], axis=0)
    rows = dot(rows, order, 1, 0)
    lane = iota((1, 128), 1)
    for c in range(16):
        packed = None
        for b in range(16):
            piece = rows[16 * b : 16 * b + 16, :]
            shift = (8 * (b - c)) % 128
            moved = roll(piece, shift) if shift else piece
            packed = moved if packed is None else jnp.where(lane // 8 == b, moved, packed)
        columns = slice(128 * c, 128 * c + 128)
        block = jnp.concatenate([value_ref[:, columns], gate_ref[:, columns], packed.astype(bf16)], axis=0)
        pack_ref[48 * c : 48 * c + 48, :] = block
    pack_ref[768:, :] = gain


def pack_rows(ref, first, count):
    base = ref.shape[0] - PACK
    return ref[base + first : base + first + count, :]


def weight_rows(packs, first):
    return jnp.concatenate(
        [stack([pack_rows(x, 48 * b + first, 16) for x in packs]) for b in range(16)],
        axis=1,
    )


def rows_kernel(x_ref, *refs):
    packs, small, rate_ref, sources, outs, held, sems = (
        refs[:8], refs[8:13], refs[13], refs[14:16], refs[16:19], refs[19:21], refs[21],
    )
    gain_ref, strength_ref, decay_ref, log_decay_ref, parent_ref = small
    probe_ref, pv_ref, gate_ref = outs
    wq_ref, wk_ref = held
    halves = [pl.ds(1024 * i, 1024) for i in range(2)]
    copies = [
        pltpu.make_async_copy(source.at[half], target.at[half], sems.at[i, j])
        for i, half in enumerate(halves)
        for j, (source, target) in enumerate(zip(sources, held))
    ]
    start_all(copies)
    group = lax.axis_index("tp")
    x = x_ref[...].astype(f32)
    scale = lax.rsqrt(jnp.mean(x * x, axis=0, keepdims=True) + epsilon)
    column = iota((128, 128), 1) == iota((128, 128), 0)
    gain = jnp.concatenate(
        [jnp.where(column, gain_ref[b : b + 1, :].astype(f32), 0.0).astype(bf16) for b in range(16)], axis=0
    )
    gain = dot(gain, jnp.ones((128, 128), bf16), 1, 0)
    normed = (x * scale * gain).astype(bf16)

    def project(weight, dim):
        return dot(weight, normed, dim, 0)

    def rounded(x):
        return x.astype(bf16).astype(f32)

    first = iota((16, 2048), 0) == 0
    scalars = jnp.where(first, strength_ref[...].astype(f32), decay_ref[...].astype(f32))
    scalars = scalars.astype(bf16)
    both = jnp.concatenate([weight_rows(packs, 0), weight_rows(packs, 16)], axis=0)
    both = rounded(project(both, 1))
    values, zgate = both[:128], both[128:]
    logits = project(scalars, 1)
    queries = keys = 0.0
    for i, half in enumerate(halves):
        wait_all(copies[2 * i : 2 * i + 2])
        part = normed[1024 * i : 1024 * i + 1024]
        queries = queries + dot(wq_ref[half, :], part, 0, 0)
        keys = keys + dot(wk_ref[half, :], part, 0, 0)
    queries, keys = rounded(queries), rounded(keys)
    gain = jnp.concatenate([pack_rows(pack, 768, 16) for pack in packs], axis=0).astype(f32)

    def unit(x):
        return x * lax.rsqrt(jnp.sum(x * x, axis=0, keepdims=True) + epsilon)

    queries = unit(queries) * 128**-0.5
    keys = unit(keys)
    beta = jax.nn.sigmoid(logits[0:1, :])
    pre = logits[1:2, :]
    softplus = jnp.maximum(pre, 0.0) + jnp.log1p(jnp.exp(-jnp.abs(pre)))
    log_decay = chunk_lanes([log_decay_ref[i] for i in range(4)], group)
    parent = chunk_lanes([parent_ref[i : i + 1, :].astype(f32) for i in range(4)], group)
    g = log_decay - rate_ref[0, 0] * softplus
    place = (iota((1, 128), 1) // 32).astype(f32)
    hit = {d: jnp.where((parent == place - d) & (place >= d), 1.0, 0.0) for d in (1, 2, 3)}
    seen = {1: hit[1]}
    seen[2] = hit[2] + hit[1] * roll(seen[1], 32)
    seen[3] = hit[3] + hit[1] * roll(seen[2], 32) + hit[2] * roll(seen[1], 64)
    gam = g + sum(seen[d] * roll(g, 32 * d) for d in (1, 2, 3))
    coupling, reach = {}, {0: jnp.sum(queries * keys, axis=0, keepdims=True)}
    for d in (1, 2, 3):
        earlier = roll(keys, 32 * d)
        weight = jnp.exp(jnp.minimum(gam - roll(gam, 32 * d), 0.0)) * seen[d]
        coupling[d] = beta * weight * jnp.sum(keys * earlier, axis=0, keepdims=True)
        reach[d] = weight * jnp.sum(queries * earlier, axis=0, keepdims=True)
    solved_values = solve(beta * values, coupling)
    solved_keys = solve((beta * jnp.exp(gam)) * keys, coupling)

    def reached(x):
        return reach[0] * x + sum(reach[d] * roll(x, 32 * d) for d in (1, 2, 3))

    probe = jnp.exp(gam) * queries - reached(solved_keys)
    probe_ref[...] = probe.astype(bf16)
    pv_ref[...] = reached(solved_values)
    gate_ref[...] = gain * (zgate * jax.nn.sigmoid(zgate))


def row_side(x, packs, small, rate, *weights):
    return pl.pallas_call(
        rows_kernel,
        in_specs=vmem_specs(14) + [pl.BlockSpec(memory_space=pltpu.SMEM)] + hbm_specs(2),
        out_specs=vmem_specs(3),
        out_shape=[
            pltpu.VMEM((128, 128), bf16),
            pltpu.VMEM((128, 128), f32),
            pltpu.VMEM((128, 128), f32),
        ],
        scratch_shapes=[pltpu.VMEM(w.shape, w.dtype) for w in weights] + [pltpu.SemaphoreType.DMA((2, 2))],
        cost_estimate=cost(2000000000, 4 << 20),
        compiler_params=pltpu.CompilerParams(vmem_limit_bytes=VMEM_LIMIT),
        name="row_side",
    )(x, *packs, *small, rate, *in_hbm(weights))


def readout_kernel(probe_ref, pv_ref, gate_ref, *rest):
    packs, states, out_ref = rest[:8], rest[8:16], rest[16]
    core = lax.rem(lax.axis_index("tp"), 2)
    own = iota((32, 16, 128), 0) == iota((32, 16, 128), 2) % 32
    pieces = []
    for state in states:
        block = state[pl.ds(pl.multiple_of(512 * core, 512), 512), :]
        read = dot(block, probe_ref[...], 1, 0)
        pieces.append(jnp.sum(jnp.where(own, read.reshape(32, 16, 128), 0.0), axis=0))
    o = jnp.concatenate(pieces, axis=0) + pv_ref[...]
    o = o * lax.rsqrt(jnp.mean(o * o, axis=0, keepdims=True) + epsilon)
    o = (o * gate_ref[...]).astype(bf16)
    out_ref[...] = dot(o, weight_rows(packs, 32), 0, 0).astype(bf16)


def readout(probe, pv, gate, packs, states):
    return pl.pallas_call(
        readout_kernel,
        in_specs=vmem_specs(19),
        out_specs=pl.BlockSpec(memory_space=pltpu.VMEM),
        out_shape=pltpu.VMEM((128, 2048), bf16),
        cost_estimate=cost(500000000, 3 << 20),
        compiler_params=pltpu.CompilerParams(vmem_limit_bytes=VMEM_LIMIT),
        name="readout",
    )(probe, pv, gate, *packs, *states)


def total_kernel(part_ref, out_ref):
    total = jnp.sum(part_ref[...].astype(f32), axis=0)
    total = total * lax.rsqrt(jnp.mean(total * total, axis=1, keepdims=True) + epsilon)
    stacked = jnp.concatenate([total[:, 128 * c : 128 * c + 128] for c in range(16)], axis=0)
    out_ref[...] = stacked.T


def sum_heads(parts):
    return pl.pallas_call(
        total_kernel,
        in_specs=vmem_specs(1),
        out_specs=pl.BlockSpec(memory_space=pltpu.VMEM),
        out_shape=pltpu.VMEM((128, 128), f32),
        cost_estimate=cost(1000000, 1 << 19),
        compiler_params=pltpu.CompilerParams(vmem_limit_bytes=VMEM_LIMIT),
        name="sum_heads",
    )(parts)


def final_kernel(x_ref, gain_ref, out_ref, scratch):
    place = iota((128, 16), 0) // 8 == iota((128, 16), 1)
    gain = jnp.sum(jnp.where(place, gain_ref[...].astype(f32), 0.0), axis=1, keepdims=True)
    scratch[...] = x_ref[...].T * gain
    lane = iota((1, 128), 1)
    rows = [scratch[pl.ds(r, 16, 8), :] for r in range(8)]
    blocks = []
    for i in range(4):
        halves = []
        for h in range(2):
            packed = None
            for q in range(4):
                shift = (32 * q - 32 * i) % 128
                moved = roll(rows[4 * h + q], shift) if shift else rows[4 * h + q]
                packed = moved if packed is None else jnp.where(lane // 32 == q, moved, packed)
            halves.append(packed)
        blocks.append(jnp.concatenate(halves, axis=1))
    full = jnp.concatenate(blocks, axis=0).astype(bf16)
    source = iota((256, 256), 0)
    target = iota((256, 256), 1)
    wanted = (source % 8) * 32 + ((source // 8) % 4) * 8 + source // 32
    order = jnp.where(wanted == target, 1.0, 0.0).astype(bf16)
    out_ref[...] = dot(full, order, 1, 0).astype(bf16).reshape(4, 16, 256)


def final_rows(x, gain):
    return pl.pallas_call(
        final_kernel,
        in_specs=vmem_specs(2),
        out_specs=pl.BlockSpec(memory_space=pltpu.VMEM),
        out_shape=jax.ShapeDtypeStruct((4, 16, 256), bf16),
        scratch_shapes=[pltpu.VMEM((128, 128), f32)],
        cost_estimate=cost(10000000, 1 << 18),
        compiler_params=pltpu.CompilerParams(vmem_limit_bytes=VMEM_LIMIT),
        name="final_rows",
    )(x, gain)


def chip_permute(x, d):
    return lax.ppermute(x, "tp", [((i + 2 * d) % 8, i) for i in range(8)])


def core_permute(x):
    return lax.ppermute(x, "tp", [(i ^ 1, i) for i in range(8)])


def whole_step(
    tokens,
    input_norm_gain,
    query_weight,
    key_weight,
    value_weight,
    output_gate_weight,
    strength_weight,
    decay_weight,
    head_decay_rate,
    proposal_log_decay,
    head_norm_gain,
    output_weight,
    output_norm_gain,
    state,
    previous_keys,
    previous_values,
    previous_log_decay,
    previous_strengths,
    accepted,
    parent,
):
    sent, pack, bundle, *ahead, other_rows = prepare(
        (
            jnp.transpose(tokens, (1, 2, 0)),
            jnp.transpose(value_weight[:, 0, :], (1, 0)),
            jnp.transpose(output_gate_weight[:, 0, :], (1, 0)),
            output_weight[0],
            head_norm_gain.reshape(1, 16),
        ),
        (
            previous_keys.reshape(1024, 128),
            jnp.transpose(previous_values[:, :, 0, :], (1, 2, 0)),
            jnp.transpose(previous_strengths, (1, 2, 0)),
            jnp.transpose(previous_log_decay, (1, 2, 0)),
            accepted.reshape(1, 256),
            input_norm_gain.reshape(16, 128),
            jnp.transpose(strength_weight, (1, 0)),
            jnp.transpose(decay_weight, (1, 0)),
            jnp.transpose(proposal_log_decay, (1, 2, 0)),
            jnp.transpose(parent, (1, 0)),
        ),
        state.reshape(256, 16, 128),
    )
    ahead, small = ahead[:5], ahead[5:]
    near = [pack, chip_permute(pack, 1), chip_permute(bundle, 2), chip_permute(pack, 3)]
    x = lax.all_to_all(sent.reshape(128, 16, 128), BOTH, 0, 0, tiled=True).reshape(2048, 128)
    lows = other_chips_state(other_rows, ahead)
    accepted_state, own_low = all_chips_state(state.reshape(256, 16, 128), previous_keys.reshape(1024, 128), ahead[1:])
    one, three = chip_permute(lows[1], 1), chip_permute(lows[0], 3)
    packs = near + [core_permute(x) for x in near]
    partner_low = core_permute(own_low)
    states = [own_low, one, near[2], three, partner_low, core_permute(one), packs[6], core_permute(three)]
    rows = row_side(x, packs, small, head_decay_rate.reshape(1, 1), query_weight, key_weight)
    part = readout(*rows, packs, states)
    parts = lax.all_to_all(part.reshape(16, 8, 2048), "kv", 0, 0, tiled=True)
    blocks = lax.all_to_all(sum_heads(parts), BOTH, 0, 0, tiled=True)
    out = final_rows(blocks, output_norm_gain.reshape(1, 16))
    return jnp.transpose(out, (2, 0, 1)), accepted_state.reshape(state.shape)


def solution(mesh):
    placed = (
        P(None, None, ("kv", "tp")),
        P(),
        P(None, "kv"),
        P(None, "kv"),
        P(None, "kv", "tp"),
        P(None, "kv", "tp"),
        P(None, "kv"),
        P(None, "kv"),
        P("kv"),
        P(None, None, "kv"),
        P("tp"),
        P("kv", "tp", None),
        P(("kv", "tp")),
        P(None, "kv", "tp", None),
        P(None, None, "kv"),
        P(None, None, "kv", "tp"),
        P(None, None, "kv"),
        P(None, None, "kv"),
        P(),
        P(),
    )
    return jax.shard_map(
        whole_step,
        mesh=mesh,
        in_specs=placed,
        out_specs=(P(None, None, ("kv", "tp")), P(None, "kv", "tp", None)),
        check_vma=False,
    )
```
